512 devices in a mesh: ep: 32 (over z, core), tp: 16 (over y, x).
Axes of the slice: x: 4, y: 4, z: 16, core: 2. Of those that a mesh axis runs over, the one named last changes fastest.
Arguments:
- query_proj: bfloat16 [16384, 1024], P('ep', 'tp'), may hold values from -6 to 6
- key_proj: bfloat16 [16384, 256], P('ep'), may hold values from -6 to 6
- value_proj: bfloat16 [16384, 256], P('ep'), may hold values from -24 to 24
- sink_logit: float32 [16], P('tp'), may hold values from 2 to 6
- out_weight: bfloat16 [1024, 2048], P(None, 'tp'), may hold values from -0.1875 to 0.1875
- expert_input: bfloat16 [8192, 2048], P('ep'), may hold values from -6 to 6
- norm_gain: float32 [2048], replicated, may hold values from 0.1 to 1.9
- routes: int32 [8192, 2], P('ep'), may hold values from 0 to 31, as said below
- route_weights: float32 [8192, 2], P('ep'), may hold values from 0.2 to 1
- gate_weight: bfloat16 [32, 2048, 4096], P('ep', None, 'tp'), may hold values from -0.125 to 0.125
- up_weight: bfloat16 [32, 2048, 4096], P('ep', None, 'tp'), may hold values from -0.125 to 0.125
- down_weight: bfloat16 [32, 4096, 2048], P('ep', 'tp'), may hold values from -0.09375 to 0.09375
Outputs:
- mixer_out: bfloat16 [16384, 2048], P('ep', 'tp')
- expert_out: bfloat16 [8192, 2048], P('ep', 'tp')
The draws below stay inside these ranges and needn't reach their ends.
Inputs may be any that keep to these rules, and one draw needn't show every extreme that they name: `routes`: experts form 4 groups of consecutive numbers of equal size. Each row names 2 different experts of one group. In each aligned block of 256 rows no expert is named by more than 32 rows, and in every block some expert is named by exactly 32 rows.
All inputs are finite; a program needn't handle non-finite values.
Results may differ from the reference program's by a relative error of at most 0.017.
Values may be sent and summed in bfloat16 or wider, within the bound.
No kernel may reach another device: no remote copies, remote signals or barrier semaphores. Data moves between devices by JAX's collectives and lax.ppermute only.
A program may use at most 64 MiB of HBM per device.

```python
import jax
import jax.numpy as jnp
from jax import lax

D = 2048
HEADS = 16
KV_HEADS = 4
HEAD_DIM = 64
HALF_WIN = 128
ROWS_B = 256
TOK_A = 16384
TOK_B = 8192
EXPERTS = 32
GROUPS = 4
TOP_K = 2
EXP_HID = 4096
CAP = 32
N_TP = 16


def drawn_pair(key):
    base_key = jax.random.fold_in(key, 7)
    key_rows = jax.random.normal(jax.random.fold_in(base_key, 1), (TOK_A, KV_HEADS * HEAD_DIM), jnp.float32)
    query_rows = jax.random.normal(jax.random.fold_in(base_key, 2), (TOK_A, HEADS * HEAD_DIM), jnp.float32)
    return (jnp.clip(query_rows, -6.0, 6.0), jnp.clip(key_rows, -6.0, 6.0))


def draw_query_proj(key, part):
    return drawn_pair(key)[0].astype(jnp.bfloat16)


def draw_key_proj(key, part):
    return drawn_pair(key)[1].astype(jnp.bfloat16)


def draw_routes(key, part):
    per_group = EXPERTS // GROUPS
    block_count = TOK_B // ROWS_B
    base_key = jax.random.fold_in(key, 31)
    busy_group = jax.random.randint(jax.random.fold_in(base_key, 1), (block_count, 1), 0, GROUPS)
    other_step = jax.random.randint(jax.random.fold_in(base_key, 2), (block_count, ROWS_B), 1, GROUPS)
    order_keys = jax.random.split(jax.random.fold_in(base_key, 3), block_count)
    row_order = jax.vmap(lambda sub_key: jax.random.permutation(sub_key, ROWS_B))(order_keys)
    in_busy = row_order < ROWS_B // 2
    group_ids = jnp.where(in_busy, busy_group, (busy_group + other_step) % GROUPS)
    onehot = (group_ids[:, :, None] == jnp.arange(GROUPS, dtype=jnp.int32)[None, None, :]).astype(jnp.int32)
    group_rank = jnp.sum((jnp.cumsum(onehot, axis=1) - onehot) * onehot, axis=2)
    offsets = jax.random.randint(jax.random.fold_in(base_key, 4), (block_count, GROUPS), 0, per_group)
    shifts = jax.random.randint(jax.random.fold_in(base_key, 5), (block_count, GROUPS), 1, per_group)
    offset_row = jnp.take_along_axis(offsets, group_ids, axis=1)
    shift_row = jnp.take_along_axis(shifts, group_ids, axis=1)
    first_pick = (group_rank + offset_row) % per_group
    second_pick = (group_rank + offset_row + shift_row) % per_group
    chosen = group_ids[:, :, None] * per_group + jnp.stack([first_pick, second_pick], axis=-1)
    return chosen.reshape(TOK_B, TOP_K).astype(jnp.int32)


def block_levels(stream_key, dims, cuts, low, top_value):
    loudness = 1.0
    for axis_at, blocks in cuts:
        draws = jax.random.uniform(jax.random.fold_in(jax.random.fold_in(stream_key, 6), axis_at), (blocks,), jnp.float32, low / len(cuts), top_value / len(cuts))
        loudness = loudness * jnp.repeat(jnp.exp(draws), dims[axis_at] // blocks).reshape((-1,) + (1,) * (len(dims) - 1 - axis_at))
    return loudness


def centred(own_key, extent, spread, bound, cuts=(), held_as=jnp.bfloat16):
    result = spread * jax.random.normal(own_key, extent, jnp.float32)
    if cuts:
        result = result * block_levels(own_key, extent, cuts, -0.22, 0.18)
    return jnp.clip(result, -bound, bound).astype(held_as)


def setup_inputs(seed: int = 0) -> dict:
    splits = jax.random.split(jax.random.key(seed), 13)
    query_proj = draw_query_proj(jax.random.fold_in(splits[12], 71), 0)
    key_proj = draw_key_proj(jax.random.fold_in(splits[12], 71), 0)
    value_proj = centred(splits[2], (TOK_A, KV_HEADS * HEAD_DIM), 4.0, 24.0, ((0, 32),))
    sink_logit = jnp.clip(2.0 + 4.0 * jax.random.uniform(splits[3], (HEADS,), jnp.float32) ** block_levels(splits[3], (HEADS,), ((0, 16),), -0.2, 0.2), 2.0, 6.0)
    out_weight = centred(splits[4], (HEADS * HEAD_DIM, D), (HEADS * HEAD_DIM) ** -0.5, 0.1875, ((1, 16),))
    expert_input = centred(splits[5], (TOK_B, D), 1.0, 6.0, ((0, 32),))
    norm_gain = jnp.clip(1.0 + 0.18 * jax.random.normal(splits[6], (D,), jnp.float32), 0.1, 1.9)
    routes = draw_routes(jax.random.fold_in(splits[12], 71), 0)
    route_weights = jnp.clip(0.2 + 0.8 * jax.random.uniform(splits[8], (TOK_B, TOP_K), jnp.float32) ** block_levels(splits[8], (TOK_B, TOP_K), ((0, 32),), -0.2, 0.2), 0.2, 1.0)
    gate_weight = centred(splits[9], (EXPERTS, D, EXP_HID), D ** -0.5, 0.125, ((0, 32), (2, 16)))
    up_weight = centred(splits[10], (EXPERTS, D, EXP_HID), D ** -0.5, 0.125, ((0, 32), (2, 16)))
    down_weight = centred(splits[11], (EXPERTS, EXP_HID, D), EXP_HID ** -0.5, 0.09375, ((0, 32), (1, 16)))
    return dict(query_proj=query_proj, key_proj=key_proj, value_proj=value_proj, sink_logit=sink_logit, out_weight=out_weight, expert_input=expert_input, norm_gain=norm_gain, routes=routes, route_weights=route_weights, gate_weight=gate_weight, up_weight=up_weight, down_weight=down_weight)


NORM_EPS = 1e-06
ROPE_BASE = 10000.0
NEG_BIG = -1e+30

def rotate(features, position_start):
    count = features.shape[0]
    half_dim = features.shape[-1] // 2
    inverse_freq = 1.0 / ROPE_BASE ** (jnp.arange(half_dim, dtype=jnp.float32) * 2.0 / features.shape[-1])
    position = (jnp.arange(count, dtype=jnp.int32) + position_start).astype(jnp.float32)
    angles = position[:, None] * inverse_freq[None, :]
    cosine = jnp.cos(angles)[:, None, :]
    sine_part = jnp.sin(angles)[:, None, :]
    lower_half = features[..., :half_dim]
    upper_half = features[..., half_dim:]
    return jnp.concatenate([lower_half * cosine - upper_half * sine_part, upper_half * cosine + lower_half * sine_part], axis=-1)

def attention_ref(query_proj, key_proj, value_proj, sink_logit):
    seq_total = query_proj.shape[0]
    per_kv = HEADS // KV_HEADS
    rot_q = rotate(query_proj.reshape(seq_total, HEADS, HEAD_DIM).astype(jnp.float32), 0).astype(jnp.bfloat16)
    rot_k = rotate(key_proj.reshape(seq_total, KV_HEADS, HEAD_DIM).astype(jnp.float32), 0).astype(jnp.bfloat16)
    padding = ((HALF_WIN, HALF_WIN), (0, 0), (0, 0))
    padded_k = jnp.pad(rot_k, padding)
    padded_v = jnp.pad(value_proj.reshape(seq_total, KV_HEADS, HEAD_DIM), padding)
    grouped_sink = sink_logit.reshape(KV_HEADS, per_kv)
    block_rows = min(512, seq_total)
    key_rows = block_rows + 2 * HALF_WIN

    def one_block(block_index):
        start_row = block_index * block_rows
        query_block = lax.dynamic_slice_in_dim(rot_q, start_row, block_rows, 0).reshape(block_rows, KV_HEADS, per_kv, HEAD_DIM).astype(jnp.float32)
        key_block = lax.dynamic_slice_in_dim(padded_k, start_row, key_rows, 0).astype(jnp.float32)
        value_block = lax.dynamic_slice_in_dim(padded_v, start_row, key_rows, 0).astype(jnp.float32)
        scores = jnp.einsum('qngd,knd->ngqk', query_block, key_block) * HEAD_DIM ** (-0.5)
        key_offset = jnp.arange(key_rows, dtype=jnp.int32) - HALF_WIN
        key_gap = key_offset[None, :] - jnp.arange(block_rows, dtype=jnp.int32)[:, None]
        global_key = start_row + key_offset
        allowed = (jnp.abs(key_gap) <= HALF_WIN) & (global_key >= 0)[None, :] & (global_key < seq_total)[None, :]
        scores = jnp.where(allowed[None, None], scores, NEG_BIG)
        row_peak = jnp.maximum(lax.optimization_barrier(jnp.max(scores, axis=-1)), grouped_sink[:, :, None])
        lifted = jnp.exp(scores - row_peak[..., None])
        norm_total = lax.optimization_barrier(jnp.sum(lifted, axis=-1)) + jnp.exp(grouped_sink[:, :, None] - row_peak)
        probs = (lifted / norm_total[..., None]).astype(jnp.bfloat16)
        weighted = jnp.einsum('ngqk,knd->qngd', probs.astype(jnp.float32), value_block)
        return weighted.astype(jnp.bfloat16).reshape(block_rows, HEADS * HEAD_DIM)
    blocks = lax.map(one_block, jnp.arange(seq_total // block_rows, dtype=jnp.int32))
    return blocks.reshape(seq_total, HEADS * HEAD_DIM)

def experts_ref(expert_input, norm_gain, routes, route_weights, gate_weight, up_weight, down_weight):
    widened = expert_input.astype(jnp.float32)
    normed = (widened * lax.rsqrt(lax.optimization_barrier(jnp.mean(widened * widened, axis=1, keepdims=True)) + NORM_EPS) * norm_gain).astype(jnp.bfloat16)
    block_count = TOK_B // ROWS_B
    flat_routes = routes.reshape(block_count, ROWS_B * TOP_K)
    onehot = (flat_routes[:, :, None] == jnp.arange(EXPERTS, dtype=jnp.int32)[None, None, :]).astype(jnp.int32)
    slot_rank = lax.optimization_barrier(jnp.sum((jnp.cumsum(onehot, axis=1) - onehot) * onehot, axis=2))
    row_index = (jnp.arange(TOK_B * TOP_K, dtype=jnp.int32) // TOP_K).reshape(block_count, ROWS_B * TOP_K)
    block_index = jnp.broadcast_to(jnp.arange(block_count, dtype=jnp.int32)[:, None], flat_routes.shape)
    table = jnp.zeros((EXPERTS, block_count, CAP), jnp.int32).at[flat_routes, block_index, slot_rank].set(row_index)
    span_units = EXP_HID // N_TP

    def one_expert(operands):
        rows_table, gate_x, up_x, down_x = operands
        gathered = normed[rows_table.reshape(-1)]
        gate_sum = jnp.dot(gathered, gate_x, preferred_element_type=jnp.float32)
        up_sum = jnp.dot(gathered, up_x, preferred_element_type=jnp.float32)
        hidden = (jax.nn.silu(gate_sum) * up_sum).astype(jnp.bfloat16)
        slot_total = hidden.shape[0]
        parts = jnp.einsum('snh,nhd->nsd', hidden.reshape(slot_total, N_TP, span_units).astype(jnp.float32), down_x.reshape(N_TP, span_units, D).astype(jnp.float32)).astype(jnp.bfloat16)
        return lax.optimization_barrier(jnp.sum(parts.astype(jnp.float32), axis=0)).astype(jnp.bfloat16)
    results = lax.map(one_expert, (table, gate_weight, up_weight, down_weight))
    picked = results[flat_routes, block_index * CAP + slot_rank]
    picked = picked.reshape(TOK_B, TOP_K, D).astype(jnp.float32)
    return lax.optimization_barrier(jnp.sum(picked * route_weights[:, :, None], axis=1)).astype(jnp.bfloat16)

def reference(query_proj, key_proj, value_proj, sink_logit, out_weight, expert_input, norm_gain, routes, route_weights, gate_weight, up_weight, down_weight):
    attended = attention_ref(query_proj, key_proj, value_proj, sink_logit)
    mixer_out = jnp.dot(attended, out_weight, preferred_element_type=jnp.float32).astype(jnp.bfloat16)
    expert_out = experts_ref(expert_input, norm_gain, routes, route_weights, gate_weight, up_weight, down_weight)
    return (mixer_out, expert_out)
```

```python
import functools

import jax
import jax.numpy as jnp
from jax import lax
from jax.experimental import pallas as pl
from jax.experimental.pallas import tpu as pltpu
from jax.sharding import Mesh
from jax.sharding import PartitionSpec as P

D = 2048
HEADS = 16
KV_HEADS = 4
HEAD_DIM = 64
HALF_WIN = 128
ROWS_B = 256
EXPERTS = 32
CAP = 32
EP = ("z", "co")
TP = ("y", "x")
PLANE = ("co", "y", "x")

NORM_EPS = 1e-06
ROPE_BASE = 10000.0
NEG_BIG = -1e30

LINE_L = [[y * 4 + x for x in range(4)] for y in range(4)] + [
    [16 + y * 4 + x for y in range(4)] for x in range(4)
]
LINE_M = [[y * 4 + x for y in range(4)] for x in range(4)] + [
    [16 + y * 4 + x for x in range(4)] for y in range(4)
]
WHOLE = [list(range(16)), [16 + (p % 4) * 4 + p // 4 for p in range(16)]]

ANY = pl.BlockSpec(memory_space=pl.ANY)
VMEM = pl.BlockSpec(memory_space=pltpu.VMEM)
HALF_W = 3072


def line_shift(x, step):
    pairs = [(line[i], line[(i + step) % 4]) for line in LINE_L for i in range(4)]
    return lax.ppermute(x, PLANE, pairs)


def prep_kernel(
    x_ref, gain_ref, routes_ref, gate_ref, up_ref, down_ref,
    out_ref, slot_ref, wa_ref, wb_ref, normed_ref, sems,
):
    copies = [
        (gate_ref.at[0], wa_ref.at[pl.ds(0, 2048)]),
        (up_ref.at[0, pl.ds(0, 1024)], wa_ref.at[pl.ds(2048, 1024)]),
        (up_ref.at[0, pl.ds(1024, 1024)], wb_ref.at[pl.ds(0, 1024)]),
    ] + [
        (down_ref.at[0, :, pl.ds(c * 256, 256)], wb_ref.at[pl.ds(1024 + c * 256, 256)])
        for c in range(8)
    ]
    copies = [pltpu.make_async_copy(s, d, sems.at[i]) for i, (s, d) in enumerate(copies)]
    for copy in copies:
        copy.start()

    def norm_rows(i, carry):
        rows = pl.ds(pl.multiple_of(i * 32, 32), 32)
        wide = x_ref[rows, :].astype(jnp.float32)
        scale = lax.rsqrt(jnp.mean(wide * wide, axis=1, keepdims=True) + NORM_EPS)
        normed_ref[rows, :] = (wide * scale * gain_ref[...]).astype(jnp.bfloat16)
        return carry

    lax.fori_loop(0, ROWS_B // 32, norm_rows, 0)

    first = routes_ref[:, 0:1]
    second = routes_ref[:, 1:2]
    expert = lax.broadcasted_iota(jnp.int32, (ROWS_B, 128), 1)
    named = jnp.where((first == expert) | (second == expert), 1.0, 0.0)
    row = lax.broadcasted_iota(jnp.int32, (ROWS_B, ROWS_B), 0)
    col = lax.broadcasted_iota(jnp.int32, (ROWS_B, ROWS_B), 1)
    below = jnp.where(col < row, 1.0, 0.0).astype(jnp.bfloat16)
    above = jnp.where(row < col, 1.0, 0.0).astype(jnp.bfloat16)
    rank = jnp.dot(below, named.astype(jnp.bfloat16), preferred_element_type=jnp.float32)
    rank_a = jnp.sum(jnp.where(first == expert, rank, 0.0), axis=1, keepdims=True)
    rank_b = jnp.sum(jnp.where(second == expert, rank, 0.0), axis=1, keepdims=True)
    slot_a = first * CAP + rank_a.astype(jnp.int32)
    slot_b = second * CAP + rank_b.astype(jnp.int32)
    pair = lax.broadcasted_iota(jnp.int32, (ROWS_B, 2), 1)
    slot_ref[...] = jnp.where(pair == 0, slot_a, slot_b)

    named_t = named.T
    rank_t = jnp.dot(named_t.astype(jnp.bfloat16), above, preferred_element_type=jnp.float32)
    mark = jnp.where(named_t > 0.5, rank_t, -1.0).astype(jnp.bfloat16)
    spread = jnp.where(
        (lax.broadcasted_iota(jnp.int32, (ROWS_B, 128), 0) >> 3) == expert, 1.0, 0.0
    ).astype(jnp.bfloat16)
    mark_rows = jnp.dot(spread, mark, preferred_element_type=jnp.float32)
    xi = lax.axis_index("x")
    yi = lax.axis_index("y")
    even = ((row >> 3) & 1) == 0
    wanted = jnp.where(even, xi, yi) * 8 + (row & 7)
    pick = jnp.where(mark_rows.astype(jnp.int32) == wanted, 1.0, 0.0).astype(jnp.bfloat16)
    from_y = jnp.dot(
        pick, normed_ref[:, pl.ds(pl.multiple_of(yi * 512, 512), 512)],
        preferred_element_type=jnp.float32,
    )
    from_x = jnp.dot(
        pick, normed_ref[:, pl.ds(pl.multiple_of(xi * 512, 512), 512)],
        preferred_element_type=jnp.float32,
    )
    even_row = ((lax.broadcasted_iota(jnp.int32, (ROWS_B, 512), 0) >> 3) & 1) == 0
    out_ref[...] = jnp.where(even_row, from_y, from_x).astype(jnp.bfloat16)
    for copy in copies:
        copy.wait()


def prepare(expert_input, norm_gain, routes, gate, up, down):
    half = jax.ShapeDtypeStruct((HALF_W, 256), jnp.bfloat16)
    return pl.pallas_call(
        prep_kernel,
        out_shape=(
            jax.ShapeDtypeStruct((ROWS_B, 512), jnp.bfloat16),
            jax.ShapeDtypeStruct((ROWS_B, 2), jnp.int32),
            half,
            half,
        ),
        in_specs=[VMEM, VMEM, VMEM, ANY, ANY, ANY],
        out_specs=(VMEM, VMEM, ANY, ANY),
        scratch_shapes=[pltpu.VMEM((ROWS_B, D), jnp.bfloat16), pltpu.SemaphoreType.DMA((11,))],
        name="prep",
    )(expert_input, norm_gain.reshape(1, D), routes, gate, up, down)


def slice_hidden(x_ref, wa, wb):
    def part(m, ref, start):
        return jnp.dot(x_ref[m], ref[pl.ds(start, 512), :], preferred_element_type=jnp.float32)

    gate = part(0, wa, 0) + part(1, wa, 512) + part(2, wa, 1024) + part(3, wa, 1536)
    up = part(0, wa, 2048) + part(1, wa, 2560) + part(2, wb, 0) + part(3, wb, 512)
    return (gate / (1.0 + jnp.exp(-gate)) * up).astype(jnp.bfloat16)


def ffn_most_kernel(x_ref, *refs):
    weights, acc_ref, bufs, sems = refs[:6], refs[6], refs[7], refs[8]
    copies = [
        pltpu.make_async_copy(w, bufs.at[i], sems.at[i]) for i, w in enumerate(weights)
    ]
    for copy in copies:
        copy.start()
    for s in range(3):
        copies[2 * s].wait()
        copies[2 * s + 1].wait()
        wa, wb = bufs.at[2 * s], bufs.at[2 * s + 1]
        hidden = slice_hidden(x_ref, wa, wb)
        for c in range(8):
            cols = pl.ds(c * 256, 256)
            term = jnp.dot(
                hidden, wb[pl.ds(1024 + c * 256, 256), :], preferred_element_type=jnp.float32
            )
            acc_ref[:, cols] = term if s == 0 else acc_ref[:, cols] + term


def ffn_most(x, *weights):
    return pl.pallas_call(
        ffn_most_kernel,
        out_shape=jax.ShapeDtypeStruct((ROWS_B, D), jnp.float32),
        in_specs=[VMEM] + [ANY] * 6,
        out_specs=VMEM,
        scratch_shapes=[
            pltpu.VMEM((6, HALF_W, 256), jnp.bfloat16), pltpu.SemaphoreType.DMA((6,))
        ],
        name="ffn_most",
    )(x, *weights)


def ffn_last_kernel(x_ref, acc_ref, wa_ref, wb_ref, out_ref):
    core = lax.axis_index("co")
    hidden = slice_hidden(x_ref, wa_ref, wb_ref)
    for c in range(8):
        total = acc_ref[:, pl.ds(c * 256, 256)] + jnp.dot(
            hidden, wb_ref[pl.ds(1024 + c * 256, 256), :], preferred_element_type=jnp.float32
        )
        for k in range(2):
            t = 2 * c + k
            place = jnp.where(core == 0, t, (t % 4) * 4 + t // 4)
            out_ref[place] = total[:, k * 128 : (k + 1) * 128].astype(jnp.bfloat16)


def ffn_last(x, acc, wa, wb):
    return pl.pallas_call(
        ffn_last_kernel,
        out_shape=jax.ShapeDtypeStruct((16, ROWS_B, 128), jnp.bfloat16),
        in_specs=[VMEM] * 4,
        out_specs=VMEM,
        name="ffn_last",
    )(x, acc, wa, wb)


def combine_kernel(ret_ref, slot_ref, weight_ref, out_ref):
    place = lax.broadcasted_iota(jnp.int32, (ROWS_B, EXPERTS * CAP), 1)
    total = None
    for k in range(2):
        pick = jnp.where(place == slot_ref[:, k : k + 1], 1.0, 0.0).astype(jnp.bfloat16)
        rows = jnp.dot(pick, ret_ref[...], preferred_element_type=jnp.float32)
        term = rows * weight_ref[:, k : k + 1]
        total = term if total is None else total + term
    out_ref[...] = total.astype(jnp.bfloat16)


def combine(returned, slots, route_weights):
    return pl.pallas_call(
        combine_kernel,
        out_shape=jax.ShapeDtypeStruct((ROWS_B, 128), jnp.bfloat16),
        in_specs=[VMEM] * 3,
        out_specs=VMEM,
        name="combine",
    )(returned, slots, route_weights)


def padded(block, axis, dim, width):
    count = lax.axis_size(axis)
    forward = [(i, i + 1) for i in range(count - 1)]
    backward = [(target, source) for source, target in forward]
    low = lax.ppermute(
        lax.slice_in_dim(block, block.shape[dim] - width, None, axis=dim), axis, forward
    )
    high = lax.ppermute(lax.slice_in_dim(block, 0, width, axis=dim), axis, backward)
    return jnp.concatenate([low, block, high], axis=dim)


def collect(x, axis, dim):
    devices = lax.axis_size(axis)
    blocks = lax.all_to_all(
        jnp.broadcast_to(x[None], (devices, *x.shape)), axis, 0, 0, tiled=True
    )
    dims = list(x.shape)
    dims[dim] *= devices
    return jnp.moveaxis(blocks, 0, dim).reshape(dims)


def rotate(features, position_start):
    count = features.shape[0]
    half_dim = features.shape[-1] // 2
    inverse_freq = 1.0 / ROPE_BASE ** (
        jnp.arange(half_dim, dtype=jnp.float32) * 2.0 / features.shape[-1]
    )
    position = (jnp.arange(count, dtype=jnp.int32) + position_start).astype(jnp.float32)
    angles = position[:, None] * inverse_freq[None, :]
    cosine = jnp.cos(angles)[:, None, :]
    sine_part = jnp.sin(angles)[:, None, :]
    lower_half = features[..., :half_dim]
    upper_half = features[..., half_dim:]
    return jnp.concatenate(
        [
            lower_half * cosine - upper_half * sine_part,
            upper_half * cosine + lower_half * sine_part,
        ],
        axis=-1,
    )


def attend(query_proj, key_proj, value_proj, sink_logit):
    row_count = query_proj.shape[0]
    local_heads = query_proj.shape[1] // HEAD_DIM
    per_kv = HEADS // KV_HEADS
    kv_local = max(1, local_heads // per_kv)
    group_size = local_heads // kv_local
    tp_index = lax.axis_index(TP)
    offset = lax.axis_index(EP) * row_count
    seq_total = row_count * lax.axis_size(EP)
    first_kv = tp_index * local_heads // per_kv
    own_keys = lax.dynamic_slice_in_dim(key_proj, first_kv * HEAD_DIM, kv_local * HEAD_DIM, 1)
    own_values = lax.dynamic_slice_in_dim(value_proj, first_kv * HEAD_DIM, kv_local * HEAD_DIM, 1)
    rot_q = rotate(
        query_proj.reshape(row_count, local_heads, HEAD_DIM).astype(jnp.float32), offset
    ).astype(jnp.bfloat16)
    rot_k = rotate(
        own_keys.reshape(row_count, kv_local, HEAD_DIM).astype(jnp.float32), offset
    ).astype(jnp.bfloat16)
    stacked = jnp.stack([rot_k, own_values.reshape(row_count, kv_local, HEAD_DIM)])
    extended = padded(stacked, EP, 1, HALF_WIN)
    own_sink = sink_logit.reshape(kv_local, group_size)
    block_rows = row_count
    key_rows = block_rows + 2 * HALF_WIN
    key_offset = jnp.arange(key_rows, dtype=jnp.int32) - HALF_WIN
    key_gap = key_offset[None, :] - jnp.arange(block_rows, dtype=jnp.int32)[:, None]
    query_block = rot_q.reshape(block_rows, kv_local, group_size, HEAD_DIM)
    scores = jnp.einsum(
        "qngd,knd->ngqk", query_block, extended[0], preferred_element_type=jnp.float32
    ) * HEAD_DIM ** (-0.5)
    global_key = offset + key_offset
    allowed = (
        (jnp.abs(key_gap) <= HALF_WIN)
        & (global_key >= 0)[None, :]
        & (global_key < seq_total)[None, :]
    )
    scores = jnp.where(allowed[None, None], scores, NEG_BIG)
    row_peak = jnp.maximum(jnp.max(scores, axis=-1), own_sink[:, :, None])
    lifted = jnp.exp(scores - row_peak[..., None])
    norm_total = jnp.sum(lifted, axis=-1) + jnp.exp(own_sink[:, :, None] - row_peak)
    probs = (lifted / norm_total[..., None]).astype(jnp.bfloat16)
    weighted = jnp.einsum("ngqk,knd->qngd", probs, extended[1], preferred_element_type=jnp.float32)
    return weighted.astype(jnp.bfloat16).reshape(block_rows, local_heads * HEAD_DIM)


def local(
    query_proj,
    key_proj,
    value_proj,
    sink_logit,
    out_weight,
    expert_input,
    norm_gain,
    routes,
    route_weights,
    gate_weight,
    up_weight,
    down_weight,
):
    outgoing, slots, wa, wb = prepare(
        expert_input, norm_gain, routes, gate_weight, up_weight, down_weight
    )
    prev_a = line_shift(wa, 1)
    next_b = line_shift(wb, -1)
    next_a = line_shift(wa, -1)
    prev_b = line_shift(wb, 1)
    arrived = lax.all_to_all(outgoing, EP, 0, 0, tiled=True)
    prev_a, next_b, arrived = lax.optimization_barrier((prev_a, next_b, arrived))
    far_a = line_shift(prev_a, 1)
    far_b = line_shift(next_b, -1)

    attended = attend(query_proj, key_proj, value_proj, sink_logit)

    rows = lax.all_to_all(
        jnp.broadcast_to(arrived[None], (4, *arrived.shape)),
        PLANE, 0, 0, tiled=True, axis_index_groups=LINE_M,
    )
    acc = ffn_most(rows, wa, wb, prev_a, prev_b, next_a, next_b)
    partial = ffn_last(rows, acc, far_a, far_b)
    parts = lax.all_to_all(partial, PLANE, 0, 0, tiled=True, axis_index_groups=WHOLE)
    result = jnp.sum(parts.reshape(4, 4, EXPERTS, 8, 128).astype(jnp.float32), axis=0)
    result = jnp.moveaxis(result.astype(jnp.bfloat16), 0, 1).reshape(EXPERTS, CAP, 128)
    returned = lax.all_to_all(result, EP, 0, 0, tiled=True)
    expert_out = combine(returned.reshape(EXPERTS * CAP, 128), slots, route_weights)

    gathered = collect(attended, TP, 1)
    mixer_out = jnp.dot(gathered, out_weight, preferred_element_type=jnp.float32)
    return (mixer_out.astype(jnp.bfloat16), expert_out)


def solution(mesh):
    finer = Mesh(mesh.devices.reshape(16, 2, 4, 4), ("z", "co", "y", "x"))
    in_specs = (
        P(EP, TP),
        P(EP, None),
        P(EP, None),
        P(TP),
        P(None, TP),
        P(EP, None),
        P(),
        P(EP, None),
        P(EP, None),
        P(EP, None, TP),
        P(EP, None, TP),
        P(EP, TP, None),
    )
    out_specs = (P(EP, TP), P(EP, TP))
    return jax.shard_map(local, mesh=finer, in_specs=in_specs, out_specs=out_specs, check_vma=False)
```

```python
import functools

import jax
import jax.numpy as jnp
from jax import lax
from jax.experimental import pallas as pl
from jax.experimental.pallas import tpu as pltpu
from jax.sharding import Mesh
from jax.sharding import PartitionSpec as P

D = 2048
HEADS = 16
KV_HEADS = 4
HEAD_DIM = 64
HALF_WIN = 128
ROWS_B = 256
EXPERTS = 32
CAP = 32
EP = ("z", "co")
TP = ("y", "x")
PLANE = ("co", "y", "x")

NORM_EPS = 1e-06
ROPE_BASE = 10000.0
NEG_BIG = -1e30

LINE_L = [[y * 4 + x for x in range(4)] for y in range(4)] + [
    [16 + y * 4 + x for y in range(4)] for x in range(4)
]
LINE_M = [[y * 4 + x for y in range(4)] for x in range(4)] + [
    [16 + y * 4 + x for x in range(4)] for y in range(4)
]
WHOLE = [list(range(16)), [16 + (p % 4) * 4 + p // 4 for p in range(16)]]

ANY = pl.BlockSpec(memory_space=pl.ANY)
VMEM = pl.BlockSpec(memory_space=pltpu.VMEM)
HALF_W = 3072


def line_shift(x, step):
    pairs = [(line[i], line[(i + step) % 4]) for line in LINE_L for i in range(4)]
    return lax.ppermute(x, PLANE, pairs)


def prep_kernel(
    x_ref, gain_ref, routes_ref, gate_ref, up_ref, down_ref,
    out_ref, slot_ref, wa_ref, wb_ref, normed_ref, sa_ref, sb_ref, sems,
):
    copies = [
        (gate_ref.at[0], sa_ref.at[pl.ds(0, 2048)]),
        (up_ref.at[0, pl.ds(0, 1024)], sa_ref.at[pl.ds(2048, 1024)]),
        (up_ref.at[0, pl.ds(1024, 1024)], sb_ref.at[pl.ds(0, 1024)]),
    ] + [
        (down_ref.at[0, :, pl.ds(c * 256, 256)], sb_ref.at[pl.ds(1024 + c * 256, 256)])
        for c in range(8)
    ]
    copies = [pltpu.make_async_copy(s, d, sems.at[i]) for i, (s, d) in enumerate(copies)]
    for copy in copies:
        copy.start()

    def norm_rows(i, carry):
        rows = pl.ds(pl.multiple_of(i * 32, 32), 32)
        wide = x_ref[rows, :].astype(jnp.float32)
        scale = lax.rsqrt(jnp.mean(wide * wide, axis=1, keepdims=True) + NORM_EPS)
        normed_ref[rows, :] = (wide * scale * gain_ref[...]).astype(jnp.bfloat16)
        return carry

    lax.fori_loop(0, ROWS_B // 32, norm_rows, 0)
    for copy in copies:
        copy.wait()
    leave = [
        pltpu.make_async_copy(sa_ref, wa_ref, sems.at[11]),
        pltpu.make_async_copy(sb_ref, wb_ref, sems.at[12]),
    ]
    for copy in leave:
        copy.start()

    first = routes_ref[0:1, :]
    second = routes_ref[1:2, :]
    expert = lax.broadcasted_iota(jnp.int32, (128, ROWS_B), 0)
    row = lax.broadcasted_iota(jnp.int32, (ROWS_B, ROWS_B), 0)
    col = lax.broadcasted_iota(jnp.int32, (ROWS_B, ROWS_B), 1)
    above = jnp.where(row < col, 1.0, 0.0).astype(jnp.bfloat16)
    named = jnp.where((first == expert) | (second == expert), 1.0, 0.0)
    rank = jnp.dot(named.astype(jnp.bfloat16), above, preferred_element_type=jnp.float32)
    rank_a = jnp.sum(jnp.where(first == expert, rank, 0.0), axis=0, keepdims=True)
    rank_b = jnp.sum(jnp.where(second == expert, rank, 0.0), axis=0, keepdims=True)
    slot_a = first * CAP + rank_a.astype(jnp.int32)
    slot_b = second * CAP + rank_b.astype(jnp.int32)
    both = jnp.where(expert == 0, slot_a, slot_b).astype(jnp.float32)
    slot_ref[...] = both.T.astype(jnp.int32)

    mark = jnp.where(named > 0.5, rank, -1.0).astype(jnp.bfloat16)
    spread = jnp.where(
        (lax.broadcasted_iota(jnp.int32, (ROWS_B, 128), 0) >> 3)
        == lax.broadcasted_iota(jnp.int32, (ROWS_B, 128), 1),
        1.0,
        0.0,
    ).astype(jnp.bfloat16)
    mark_rows = jnp.dot(spread, mark, preferred_element_type=jnp.float32)
    xi = lax.axis_index("x")
    yi = lax.axis_index("y")
    even = ((row >> 3) & 1) == 0
    wanted = jnp.where(even, xi, yi) * 8 + (row & 7)
    pick = jnp.where(mark_rows.astype(jnp.int32) == wanted, 1.0, 0.0).astype(jnp.bfloat16)
    from_y = jnp.dot(
        pick, normed_ref[:, pl.ds(pl.multiple_of(yi * 512, 512), 512)],
        preferred_element_type=jnp.float32,
    )
    from_x = jnp.dot(
        pick, normed_ref[:, pl.ds(pl.multiple_of(xi * 512, 512), 512)],
        preferred_element_type=jnp.float32,
    )
    even_row = ((lax.broadcasted_iota(jnp.int32, (ROWS_B, 512), 0) >> 3) & 1) == 0
    out_ref[...] = jnp.where(even_row, from_y, from_x).astype(jnp.bfloat16)
    for copy in leave:
        copy.wait()


def prepare(expert_input, norm_gain, routes, gate, up, down):
    half = jax.ShapeDtypeStruct((HALF_W, 256), jnp.bfloat16)
    return pl.pallas_call(
        prep_kernel,
        out_shape=(
            jax.ShapeDtypeStruct((ROWS_B, 512), jnp.bfloat16),
            jax.ShapeDtypeStruct((ROWS_B, 128), jnp.int32),
            half,
            half,
        ),
        in_specs=[VMEM, VMEM, VMEM, ANY, ANY, ANY],
        out_specs=(VMEM, VMEM, ANY, ANY),
        scratch_shapes=[
            pltpu.VMEM((ROWS_B, D), jnp.bfloat16),
            pltpu.VMEM((HALF_W, 256), jnp.bfloat16),
            pltpu.VMEM((HALF_W, 256), jnp.bfloat16),
            pltpu.SemaphoreType.DMA((13,)),
        ],
        name="prep",
    )(expert_input, norm_gain.reshape(1, D), routes.T, gate, up, down)


def slice_hidden(x_ref, wa, wb):
    def part(m, ref, start):
        return jnp.dot(x_ref[m], ref[pl.ds(start, 512), :], preferred_element_type=jnp.float32)

    gate = part(0, wa, 0) + part(1, wa, 512) + part(2, wa, 1024) + part(3, wa, 1536)
    up = part(0, wa, 2048) + part(1, wa, 2560) + part(2, wb, 0) + part(3, wb, 512)
    return (gate / (1.0 + jnp.exp(-gate)) * up).astype(jnp.bfloat16)


def ffn_kernel(x_ref, attended_ref, *refs):
    weights, out_ref, acc_ref, bufs, sems = refs[:8], refs[8], refs[9], refs[10], refs[11]
    copies = [
        pltpu.make_async_copy(w, bufs.at[i], sems.at[i]) for i, w in enumerate(weights)
    ]
    for copy in copies:
        copy.start()
    core = lax.axis_index("co")
    for t in range(16):
        out_ref[t, pl.ds(256, 256), :] = attended_ref[...]
    for s in range(4):
        copies[2 * s].wait()
        copies[2 * s + 1].wait()
        wa, wb = bufs.at[2 * s], bufs.at[2 * s + 1]
        hidden = slice_hidden(x_ref, wa, wb)
        for c in range(8):
            cols = pl.ds(c * 256, 256)
            term = jnp.dot(
                hidden, wb[pl.ds(1024 + c * 256, 256), :], preferred_element_type=jnp.float32
            )
            total = term if s == 0 else acc_ref[:, cols] + term
            if s < 3:
                acc_ref[:, cols] = total
                continue
            for k in range(2):
                t = 2 * c + k
                place = jnp.where(core == 0, t, (t % 4) * 4 + t // 4)
                piece = total[:, k * 128 : (k + 1) * 128].astype(jnp.bfloat16)
                out_ref[place, pl.ds(0, 256), :] = piece


def ffn(x, attended, weights):
    return pl.pallas_call(
        ffn_kernel,
        out_shape=jax.ShapeDtypeStruct((16, 512, 128), jnp.bfloat16),
        in_specs=[VMEM, VMEM] + [ANY] * 8,
        out_specs=VMEM,
        scratch_shapes=[
            pltpu.VMEM((ROWS_B, D), jnp.float32),
            pltpu.VMEM((8, HALF_W, 256), jnp.bfloat16),
            pltpu.SemaphoreType.DMA((8,)),
        ],
        name="ffn",
    )(x, attended, *weights)


def combine_kernel(ret_ref, slot_ref, weight_ref, out_ref):
    place = lax.broadcasted_iota(jnp.int32, (ROWS_B, EXPERTS * CAP), 1)
    total = None
    for k in range(2):
        pick = jnp.where(place == slot_ref[:, k : k + 1], 1.0, 0.0).astype(jnp.bfloat16)
        rows = jnp.dot(pick, ret_ref[...], preferred_element_type=jnp.float32)
        term = rows * weight_ref[:, k : k + 1]
        total = term if total is None else total + term
    out_ref[...] = total.astype(jnp.bfloat16)


def combine(returned, slots, route_weights):
    return pl.pallas_call(
        combine_kernel,
        out_shape=jax.ShapeDtypeStruct((ROWS_B, 128), jnp.bfloat16),
        in_specs=[VMEM] * 3,
        out_specs=VMEM,
        name="combine",
    )(returned, slots, route_weights)


def padded(block, axis, dim, width):
    count = lax.axis_size(axis)
    forward = [(i, i + 1) for i in range(count - 1)]
    backward = [(target, source) for source, target in forward]
    low = lax.ppermute(
        lax.slice_in_dim(block, block.shape[dim] - width, None, axis=dim), axis, forward
    )
    high = lax.ppermute(lax.slice_in_dim(block, 0, width, axis=dim), axis, backward)
    return jnp.concatenate([low, block, high], axis=dim)


def rotate(features, position_start):
    count = features.shape[0]
    half_dim = features.shape[-1] // 2
    inverse_freq = 1.0 / ROPE_BASE ** (
        jnp.arange(half_dim, dtype=jnp.float32) * 2.0 / features.shape[-1]
    )
    position = (jnp.arange(count, dtype=jnp.int32) + position_start).astype(jnp.float32)
    angles = position[:, None] * inverse_freq[None, :]
    cosine = jnp.cos(angles)[:, None, :]
    sine_part = jnp.sin(angles)[:, None, :]
    lower_half = features[..., :half_dim]
    upper_half = features[..., half_dim:]
    return jnp.concatenate(
        [
            lower_half * cosine - upper_half * sine_part,
            upper_half * cosine + lower_half * sine_part,
        ],
        axis=-1,
    )


def attend(query_proj, key_proj, value_proj, sink_logit):
    row_count = query_proj.shape[0]
    local_heads = query_proj.shape[1] // HEAD_DIM
    per_kv = HEADS // KV_HEADS
    kv_local = max(1, local_heads // per_kv)
    group_size = local_heads // kv_local
    tp_index = lax.axis_index(TP)
    offset = lax.axis_index(EP) * row_count
    seq_total = row_count * lax.axis_size(EP)
    first_kv = tp_index * local_heads // per_kv
    own_keys = lax.dynamic_slice_in_dim(key_proj, first_kv * HEAD_DIM, kv_local * HEAD_DIM, 1)
    own_values = lax.dynamic_slice_in_dim(value_proj, first_kv * HEAD_DIM, kv_local * HEAD_DIM, 1)
    rot_q = rotate(
        query_proj.reshape(row_count, local_heads, HEAD_DIM).astype(jnp.float32), offset
    ).astype(jnp.bfloat16)
    rot_k = rotate(
        own_keys.reshape(row_count, kv_local, HEAD_DIM).astype(jnp.float32), offset
    ).astype(jnp.bfloat16)
    stacked = jnp.stack([rot_k, own_values.reshape(row_count, kv_local, HEAD_DIM)])
    extended = padded(stacked, EP, 1, HALF_WIN)
    own_sink = sink_logit.reshape(kv_local, group_size)
    block_rows = row_count
    key_rows = block_rows + 2 * HALF_WIN
    key_offset = jnp.arange(key_rows, dtype=jnp.int32) - HALF_WIN
    key_gap = key_offset[None, :] - jnp.arange(block_rows, dtype=jnp.int32)[:, None]
    query_block = rot_q.reshape(block_rows, kv_local, group_size, HEAD_DIM)
    scores = jnp.einsum(
        "qngd,knd->ngqk", query_block, extended[0], preferred_element_type=jnp.float32
    ) * HEAD_DIM ** (-0.5)
    global_key = offset + key_offset
    allowed = (
        (jnp.abs(key_gap) <= HALF_WIN)
        & (global_key >= 0)[None, :]
        & (global_key < seq_total)[None, :]
    )
    scores = jnp.where(allowed[None, None], scores, NEG_BIG)
    row_peak = jnp.maximum(jnp.max(scores, axis=-1), own_sink[:, :, None])
    lifted = jnp.exp(scores - row_peak[..., None])
    norm_total = jnp.sum(lifted, axis=-1) + jnp.exp(own_sink[:, :, None] - row_peak)
    probs = (lifted / norm_total[..., None]).astype(jnp.bfloat16)
    weighted = jnp.einsum("ngqk,knd->qngd", probs, extended[1], preferred_element_type=jnp.float32)
    return weighted.astype(jnp.bfloat16).reshape(block_rows, local_heads * HEAD_DIM)


def local(
    query_proj,
    key_proj,
    value_proj,
    sink_logit,
    out_weight,
    expert_input,
    norm_gain,
    routes,
    route_weights,
    gate_weight,
    up_weight,
    down_weight,
):
    outgoing, slots, wa, wb = prepare(
        expert_input, norm_gain, routes, gate_weight, up_weight, down_weight
    )
    prev_a = line_shift(wa, 1)
    next_b = line_shift(wb, -1)
    next_a = line_shift(wa, -1)
    prev_b = line_shift(wb, 1)
    arrived = lax.all_to_all(outgoing, EP, 0, 0, tiled=True)
    far_a = line_shift(prev_a, 1)
    far_b = line_shift(next_b, -1)

    attended = attend(query_proj, key_proj, value_proj, sink_logit)
    packed = jnp.concatenate([attended[:256], attended[256:]], axis=1)

    rows = lax.all_to_all(
        jnp.broadcast_to(arrived[None], (4, *arrived.shape)),
        PLANE, 0, 0, tiled=True, axis_index_groups=LINE_M,
    )
    partial = ffn(rows, packed, (wa, wb, prev_a, prev_b, next_a, next_b, far_a, far_b))
    parts = lax.all_to_all(partial, PLANE, 0, 0, tiled=True, axis_index_groups=WHOLE)
    parts = parts.reshape(4, 4, 512, 128)
    result = jnp.sum(parts[:, :, :256].astype(jnp.float32), axis=0).astype(jnp.bfloat16)
    result = jnp.moveaxis(result.reshape(4, EXPERTS, 8, 128), 0, 1).reshape(EXPERTS, CAP, 128)
    returned = lax.all_to_all(result, EP, 0, 0, tiled=True)
    expert_out = combine(returned.reshape(EXPERTS * CAP, 128), slots, route_weights)

    heads = parts[:, :, 256:]
    heads = jnp.where(lax.axis_index("co") == 0, heads, jnp.swapaxes(heads, 0, 1))
    heads = heads.reshape(16, 256, 2, HEAD_DIM).transpose(2, 1, 0, 3).reshape(512, 1024)
    mixer_out = jnp.dot(heads, out_weight, preferred_element_type=jnp.float32)
    return (mixer_out.astype(jnp.bfloat16), expert_out)


def solution(mesh):
    finer = Mesh(mesh.devices.reshape(16, 2, 4, 4), ("z", "co", "y", "x"))
    in_specs = (
        P(EP, TP),
        P(EP, None),
        P(EP, None),
        P(TP),
        P(None, TP),
        P(EP, None),
        P(),
        P(EP, None),
        P(EP, None),
        P(EP, None, TP),
        P(EP, None, TP),
        P(EP, TP, None),
    )
    out_specs = (P(EP, TP), P(EP, TP))
    return jax.shard_map(local, mesh=finer, in_specs=in_specs, out_specs=out_specs, check_vma=False)
```

```python
import jax
import jax.numpy as jnp
from jax import lax
from jax.experimental import pallas as pl
from jax.experimental.pallas import tpu as pltpu
from jax.sharding import Mesh
from jax.sharding import PartitionSpec as P


D = 2048
HEADS = 16
KV_HEADS = 4
HEAD_DIM = 64
HALF_WIN = 128
ROWS_B = 256
EXPERTS = 32
CAP = 32
EP = ("z", "co")
TP = ("y", "x")
PLANE = ("co", "y", "x")

NORM_EPS = 1e-06
ROPE_BASE = 10000.0
NEG_BIG = -1e30

LINE_L = [[y * 4 + x for x in range(4)] for y in range(4)] + [
    [16 + y * 4 + x for y in range(4)] for x in range(4)
]
LINE_M = [[y * 4 + x for y in range(4)] for x in range(4)] + [
    [16 + y * 4 + x for x in range(4)] for y in range(4)
]
WHOLE = [list(range(16)), [16 + (p % 4) * 4 + p // 4 for p in range(16)]]

ANY = pl.BlockSpec(memory_space=pl.ANY)
VMEM = pl.BlockSpec(memory_space=pltpu.VMEM)
HALF_W = 3072


def line_shift(x, step):
    pairs = [(line[i], line[(i + step) % 4]) for line in LINE_L for i in range(4)]
    return lax.ppermute(x, PLANE, pairs)


def prep_kernel(
    x_ref, gain_ref, routes_ref, gate_ref, up_ref, down_ref,
    out_ref, slot_ref, wa_ref, wb_ref, normed_ref, sa_ref, sb_ref, sems,
):
    copies = [
        (gate_ref.at[0], sa_ref.at[pl.ds(0, 2048)]),
        (up_ref.at[0, pl.ds(0, 1024)], sa_ref.at[pl.ds(2048, 1024)]),
        (up_ref.at[0, pl.ds(1024, 1024)], sb_ref.at[pl.ds(0, 1024)]),
    ] + [
        (down_ref.at[0, :, pl.ds(c * 256, 256)], sb_ref.at[pl.ds(1024 + c * 256, 256)])
        for c in range(8)
    ]
    copies = [pltpu.make_async_copy(s, d, sems.at[i]) for i, (s, d) in enumerate(copies)]
    for copy in copies:
        copy.start()

    def norm_rows(i, carry):
        rows = pl.ds(pl.multiple_of(i * 32, 32), 32)
        wide = x_ref[rows, :].astype(jnp.float32)
        scale = lax.rsqrt(jnp.mean(wide * wide, axis=1, keepdims=True) + NORM_EPS)
        normed_ref[rows, :] = (wide * scale * gain_ref[...]).astype(jnp.bfloat16)
        return carry

    lax.fori_loop(0, ROWS_B // 32, norm_rows, 0)
    for copy in copies:
        copy.wait()
    leave = [
        pltpu.make_async_copy(sa_ref, wa_ref, sems.at[11]),
        pltpu.make_async_copy(sb_ref, wb_ref, sems.at[12]),
    ]
    for copy in leave:
        copy.start()

    first = routes_ref[0:1, :]
    second = routes_ref[1:2, :]
    expert = lax.broadcasted_iota(jnp.int32, (128, ROWS_B), 0)
    row = lax.broadcasted_iota(jnp.int32, (ROWS_B, ROWS_B), 0)
    col = lax.broadcasted_iota(jnp.int32, (ROWS_B, ROWS_B), 1)
    above = jnp.where(row < col, 1.0, 0.0).astype(jnp.bfloat16)
    named = jnp.where((first == expert) | (second == expert), 1.0, 0.0)
    rank = jnp.dot(named.astype(jnp.bfloat16), above, preferred_element_type=jnp.float32)
    rank_a = jnp.sum(jnp.where(first == expert, rank, 0.0), axis=0, keepdims=True)
    rank_b = jnp.sum(jnp.where(second == expert, rank, 0.0), axis=0, keepdims=True)
    slot_a = first * CAP + rank_a.astype(jnp.int32)
    slot_b = second * CAP + rank_b.astype(jnp.int32)
    both = jnp.where(expert == 0, slot_a, slot_b).astype(jnp.float32)
    slot_ref[...] = both.T.astype(jnp.int32)

    mark = jnp.where(named > 0.5, rank, -1.0).astype(jnp.bfloat16)
    spread = jnp.where(
        (lax.broadcasted_iota(jnp.int32, (ROWS_B, 128), 0) >> 3)
        == lax.broadcasted_iota(jnp.int32, (ROWS_B, 128), 1),
        1.0,
        0.0,
    ).astype(jnp.bfloat16)
    mark_rows = jnp.dot(spread, mark, preferred_element_type=jnp.float32)
    xi = lax.axis_index("x")
    yi = lax.axis_index("y")
    even = ((row >> 3) & 1) == 0
    wanted = jnp.where(even, xi, yi) * 8 + (row & 7)
    pick = jnp.where(mark_rows.astype(jnp.int32) == wanted, 1.0, 0.0).astype(jnp.bfloat16)
    from_y = jnp.dot(
        pick, normed_ref[:, pl.ds(pl.multiple_of(yi * 512, 512), 512)],
        preferred_element_type=jnp.float32,
    )
    from_x = jnp.dot(
        pick, normed_ref[:, pl.ds(pl.multiple_of(xi * 512, 512), 512)],
        preferred_element_type=jnp.float32,
    )
    even_row = ((lax.broadcasted_iota(jnp.int32, (ROWS_B, 512), 0) >> 3) & 1) == 0
    out_ref[...] = jnp.where(even_row, from_y, from_x).astype(jnp.bfloat16)
    for copy in leave:
        copy.wait()


def prepare(expert_input, norm_gain, routes, gate, up, down):
    half = jax.ShapeDtypeStruct((HALF_W, 256), jnp.bfloat16)
    return pl.pallas_call(
        prep_kernel,
        out_shape=(
            jax.ShapeDtypeStruct((ROWS_B, 512), jnp.bfloat16),
            jax.ShapeDtypeStruct((ROWS_B, 128), jnp.int32),
            half,
            half,
        ),
        in_specs=[VMEM, VMEM, VMEM, ANY, ANY, ANY],
        out_specs=(VMEM, VMEM, ANY, ANY),
        scratch_shapes=[
            pltpu.VMEM((ROWS_B, D), jnp.bfloat16),
            pltpu.VMEM((HALF_W, 256), jnp.bfloat16),
            pltpu.VMEM((HALF_W, 256), jnp.bfloat16),
            pltpu.SemaphoreType.DMA((13,)),
        ],
        name="prep",
    )(expert_input, norm_gain.reshape(1, D), routes.T, gate, up, down)


def slice_hidden(x_ref, wa, wb):
    def part(m, ref, start):
        return jnp.dot(
            x_ref[m, pl.ds(0, ROWS_B), :], ref[pl.ds(start, 512), :],
            preferred_element_type=jnp.float32,
        )

    gate = part(0, wa, 0) + part(1, wa, 512) + part(2, wa, 1024) + part(3, wa, 1536)
    up = part(0, wa, 2048) + part(1, wa, 2560) + part(2, wb, 0) + part(3, wb, 512)
    return (gate / (1.0 + jnp.exp(-gate)) * up).astype(jnp.bfloat16)


def ffn_kernel(x_ref, *refs):
    weights, out_ref, acc_ref, bufs, sems = refs[:8], refs[8], refs[9], refs[10], refs[11]
    copies = [
        pltpu.make_async_copy(w, bufs.at[i], sems.at[i]) for i, w in enumerate(weights)
    ]
    for copy in copies:
        copy.start()
    core = lax.axis_index("co")
    for s in range(4):
        copies[2 * s].wait()
        copies[2 * s + 1].wait()
        wa, wb = bufs.at[2 * s], bufs.at[2 * s + 1]
        hidden = slice_hidden(x_ref, wa, wb)
        for c in range(8):
            cols = pl.ds(c * 256, 256)
            term = jnp.dot(
                hidden, wb[pl.ds(1024 + c * 256, 256), :], preferred_element_type=jnp.float32
            )
            total = term if s == 0 else acc_ref[:, cols] + term
            if s < 3:
                acc_ref[:, cols] = total
                continue
            for k in range(2):
                t = 2 * c + k
                place = jnp.where(core == 0, t, (t % 4) * 4 + t // 4)
                piece = total[:, k * 128 : (k + 1) * 128].astype(jnp.bfloat16)
                out_ref[place] = piece


def ffn(x, weights):
    return pl.pallas_call(
        ffn_kernel,
        out_shape=jax.ShapeDtypeStruct((16, ROWS_B, 128), jnp.bfloat16),
        in_specs=[VMEM] + [ANY] * 8,
        out_specs=VMEM,
        scratch_shapes=[
            pltpu.VMEM((ROWS_B, D), jnp.float32),
            pltpu.VMEM((8, HALF_W, 256), jnp.bfloat16),
            pltpu.SemaphoreType.DMA((8,)),
        ],
        name="ffn",
    )(x, *weights)


def combine_kernel(ret_ref, slot_ref, weight_ref, out_ref):
    place = lax.broadcasted_iota(jnp.int32, (ROWS_B, EXPERTS * CAP), 1)
    total = None
    for k in range(2):
        pick = jnp.where(place == slot_ref[:, k : k + 1], 1.0, 0.0).astype(jnp.bfloat16)
        rows = jnp.dot(pick, ret_ref[...], preferred_element_type=jnp.float32)
        term = rows * weight_ref[:, k : k + 1]
        total = term if total is None else total + term
    out_ref[...] = total.astype(jnp.bfloat16)


def combine(returned, slots, route_weights):
    return pl.pallas_call(
        combine_kernel,
        out_shape=jax.ShapeDtypeStruct((ROWS_B, 128), jnp.bfloat16),
        in_specs=[VMEM] * 3,
        out_specs=VMEM,
        name="combine",
    )(returned, slots, route_weights)


def project_kernel(own_ref, prev_ref, next_ref, far_ref, weight_ref, out_ref, a_ref, w_ref):
    core = lax.axis_index("co")
    line = jnp.where(core == 0, lax.axis_index("x"), lax.axis_index("y"))
    w_ref[...] = jnp.zeros_like(w_ref)
    for j, (ref, step) in enumerate(((own_ref, 0), (prev_ref, 3), (next_ref, 1), (far_ref, 2))):
        source = lax.rem(line + step, 4)
        for m in range(4):
            head = jnp.where(core == 0, m * 4 + source, source * 4 + m)
            at = (4 * j + m) * 128
            weight = weight_ref[pl.ds(pl.multiple_of(head * HEAD_DIM, HEAD_DIM), HEAD_DIM), :]
            w_ref[pl.ds(at, 64), pl.ds(0, 128)] = weight
            w_ref[pl.ds(at + 64, 64), pl.ds(128, 128)] = weight
            for q in range(4):
                a_ref[pl.ds(q * 64, 64), pl.ds(at, 128)] = ref[m, :, pl.ds(q * 128, 128)]
    both = jnp.dot(a_ref[...], w_ref[...], preferred_element_type=jnp.float32)
    out_ref[pl.ds(0, 256), :] = both[:, :128].astype(jnp.bfloat16)
    out_ref[pl.ds(256, 256), :] = both[:, 128:].astype(jnp.bfloat16)


def project(own, prev, nxt, far, out_weight):
    return pl.pallas_call(
        project_kernel,
        out_shape=jax.ShapeDtypeStruct((512, 128), jnp.bfloat16),
        in_specs=[VMEM] * 5,
        out_specs=VMEM,
        scratch_shapes=[
            pltpu.VMEM((256, 2048), jnp.bfloat16), pltpu.VMEM((2048, 256), jnp.bfloat16)
        ],
        name="project",
    )(own, prev, nxt, far, out_weight)


def padded(block, axis, dim, width):
    count = lax.axis_size(axis)
    forward = [(i, i + 1) for i in range(count - 1)]
    backward = [(target, source) for source, target in forward]
    low = lax.ppermute(
        lax.slice_in_dim(block, block.shape[dim] - width, None, axis=dim), axis, forward
    )
    high = lax.ppermute(lax.slice_in_dim(block, 0, width, axis=dim), axis, backward)
    return jnp.concatenate([low, block, high], axis=dim)


def rotate(features, position_start):
    count = features.shape[0]
    half_dim = features.shape[-1] // 2
    inverse_freq = 1.0 / ROPE_BASE ** (
        jnp.arange(half_dim, dtype=jnp.float32) * 2.0 / features.shape[-1]
    )
    position = (jnp.arange(count, dtype=jnp.int32) + position_start).astype(jnp.float32)
    angles = position[:, None] * inverse_freq[None, :]
    cosine = jnp.cos(angles)[:, None, :]
    sine_part = jnp.sin(angles)[:, None, :]
    lower_half = features[..., :half_dim]
    upper_half = features[..., half_dim:]
    return jnp.concatenate(
        [
            lower_half * cosine - upper_half * sine_part,
            upper_half * cosine + lower_half * sine_part,
        ],
        axis=-1,
    )


def attend(query_proj, key_proj, value_proj, sink_logit):
    row_count = query_proj.shape[0]
    local_heads = query_proj.shape[1] // HEAD_DIM
    per_kv = HEADS // KV_HEADS
    kv_local = max(1, local_heads // per_kv)
    group_size = local_heads // kv_local
    tp_index = lax.axis_index(TP)
    offset = lax.axis_index(EP) * row_count
    seq_total = row_count * lax.axis_size(EP)
    first_kv = tp_index * local_heads // per_kv
    own_keys = lax.dynamic_slice_in_dim(key_proj, first_kv * HEAD_DIM, kv_local * HEAD_DIM, 1)
    own_values = lax.dynamic_slice_in_dim(value_proj, first_kv * HEAD_DIM, kv_local * HEAD_DIM, 1)
    rot_q = rotate(
        query_proj.reshape(row_count, local_heads, HEAD_DIM).astype(jnp.float32), offset
    ).astype(jnp.bfloat16)
    rot_k = rotate(
        own_keys.reshape(row_count, kv_local, HEAD_DIM).astype(jnp.float32), offset
    ).astype(jnp.bfloat16)
    stacked = jnp.stack([rot_k, own_values.reshape(row_count, kv_local, HEAD_DIM)])
    extended = padded(stacked, EP, 1, HALF_WIN)
    own_sink = sink_logit.reshape(kv_local, group_size)
    block_rows = row_count
    key_rows = block_rows + 2 * HALF_WIN
    key_offset = jnp.arange(key_rows, dtype=jnp.int32) - HALF_WIN
    key_gap = key_offset[None, :] - jnp.arange(block_rows, dtype=jnp.int32)[:, None]
    query_block = rot_q.reshape(block_rows, kv_local, group_size, HEAD_DIM)
    scores = jnp.einsum(
        "qngd,knd->ngqk", query_block, extended[0], preferred_element_type=jnp.float32
    ) * HEAD_DIM ** (-0.5)
    global_key = offset + key_offset
    allowed = (
        (jnp.abs(key_gap) <= HALF_WIN)
        & (global_key >= 0)[None, :]
        & (global_key < seq_total)[None, :]
    )
    scores = jnp.where(allowed[None, None], scores, NEG_BIG)
    row_peak = jnp.maximum(jnp.max(scores, axis=-1), own_sink[:, :, None])
    lifted = jnp.exp(scores - row_peak[..., None])
    norm_total = jnp.sum(lifted, axis=-1) + jnp.exp(own_sink[:, :, None] - row_peak)
    probs = (lifted / norm_total[..., None]).astype(jnp.bfloat16)
    weighted = jnp.einsum("ngqk,knd->qngd", probs, extended[1], preferred_element_type=jnp.float32)
    return weighted.astype(jnp.bfloat16).reshape(block_rows, local_heads * HEAD_DIM)


def local(
    query_proj,
    key_proj,
    value_proj,
    sink_logit,
    out_weight,
    expert_input,
    norm_gain,
    routes,
    route_weights,
    gate_weight,
    up_weight,
    down_weight,
):
    outgoing, slots, wa, wb = prepare(
        expert_input, norm_gain, routes, gate_weight, up_weight, down_weight
    )
    prev_a = line_shift(wa, 1)
    next_b = line_shift(wb, -1)
    next_a = line_shift(wa, -1)
    prev_b = line_shift(wb, 1)
    arrived = lax.all_to_all(outgoing, EP, 0, 0, tiled=True)
    far_a = line_shift(prev_a, 1)
    far_b = line_shift(next_b, -1)

    attended = attend(query_proj, key_proj, value_proj, sink_logit)
    packed = jnp.concatenate([attended[:256], attended[256:]], axis=1)
    packed = jnp.concatenate([packed[q * 64 : (q + 1) * 64] for q in range(4)], axis=1)

    payload = jnp.concatenate([arrived, packed], axis=0)
    rows = lax.all_to_all(
        jnp.broadcast_to(payload[None], (4, *payload.shape)),
        PLANE, 0, 0, tiled=True, axis_index_groups=LINE_M,
    )
    partial = ffn(rows, (wa, wb, prev_a, prev_b, next_a, next_b, far_a, far_b))
    parts = lax.all_to_all(partial, PLANE, 0, 0, tiled=True, axis_index_groups=WHOLE)
    parts = parts.reshape(4, 4, 256, 128)
    result = jnp.sum(parts.astype(jnp.float32), axis=0).astype(jnp.bfloat16)
    result = jnp.moveaxis(result.reshape(4, EXPERTS, 8, 128), 0, 1)
    result = result.reshape(EXPERTS, CAP, 128)
    returned = lax.all_to_all(result, EP, 0, 0, tiled=True)
    expert_out = combine(returned.reshape(EXPERTS * CAP, 128), slots, route_weights)

    heads = rows[:, 256:]
    around = [line_shift(heads, step) for step in (1, -1, 2)]
    mixer_out = project(heads, *around, out_weight)
    return (mixer_out, expert_out)


def solution(mesh):
    finer = Mesh(mesh.devices.reshape(16, 2, 4, 4), ("z", "co", "y", "x"))
    in_specs = (
        P(EP, TP),
        P(EP, None),
        P(EP, None),
        P(TP),
        P(None, TP),
        P(EP, None),
        P(),
        P(EP, None),
        P(EP, None),
        P(EP, None, TP),
        P(EP, None, TP),
        P(EP, TP, None),
    )
    out_specs = (P(EP, TP), P(EP, TP))
    return jax.shard_map(local, mesh=finer, in_specs=in_specs, out_specs=out_specs, check_vma=False)
```

```python
import jax
import jax.numpy as jnp
from jax import lax
from jax.experimental import pallas as pl
from jax.experimental.pallas import tpu as pltpu
from jax.sharding import Mesh
from jax.sharding import PartitionSpec as P


D = 2048
HEADS = 16
KV_HEADS = 4
HEAD_DIM = 64
HALF_WIN = 128
ROWS_B = 256
EXPERTS = 32
CAP = 32
EP = ("z", "co")
TP = ("y", "x")
PLANE = ("co", "y", "x")

NORM_EPS = 1e-06
ROPE_BASE = 10000.0
NEG_BIG = -1e30

LINE_L = [[y * 4 + x for x in range(4)] for y in range(4)] + [
    [16 + y * 4 + x for y in range(4)] for x in range(4)
]
LINE_M = [[y * 4 + x for y in range(4)] for x in range(4)] + [
    [16 + y * 4 + x for x in range(4)] for y in range(4)
]
WHOLE = [list(range(16)), [16 + (p % 4) * 4 + p // 4 for p in range(16)]]

ANY = pl.BlockSpec(memory_space=pl.ANY)
VMEM = pl.BlockSpec(memory_space=pltpu.VMEM)
HALF_W = 3072


def resident(x):
    return pltpu.with_memory_space_constraint(x, pltpu.VMEM)


def vmem_mib(count):
    return pltpu.CompilerParams(vmem_limit_bytes=count << 20)


def line_shift(x, step):
    pairs = [(line[i], line[(i + step) % 4]) for line in LINE_L for i in range(4)]
    return lax.ppermute(x, PLANE, pairs)


def pack_kernel(gate_ref, up_ref, wa_ref, stage_ref, sems):
    copies = [
        pltpu.make_async_copy(gate_ref.at[0], stage_ref.at[pl.ds(0, 2048)], sems.at[0]),
        pltpu.make_async_copy(
            up_ref.at[0, pl.ds(0, 1024)], stage_ref.at[pl.ds(2048, 1024)], sems.at[1]
        ),
    ]
    leave = [
        pltpu.make_async_copy(
            stage_ref.at[pl.ds(0, 2048)], wa_ref.at[pl.ds(0, 2048)], sems.at[2]
        ),
        pltpu.make_async_copy(
            stage_ref.at[pl.ds(2048, 1024)], wa_ref.at[pl.ds(2048, 1024)], sems.at[3]
        ),
    ]
    for copy in copies:
        copy.start()
    for come, go in zip(copies, leave):
        come.wait()
        go.start()
    for go in leave:
        go.wait()


def pack(gate, up):
    return pl.pallas_call(
        pack_kernel,
        out_shape=jax.ShapeDtypeStruct((HALF_W, 256), jnp.bfloat16),
        in_specs=[ANY, ANY],
        out_specs=ANY,
        scratch_shapes=[
            pltpu.VMEM((HALF_W, 256), jnp.bfloat16), pltpu.SemaphoreType.DMA((4,))
        ],
        compiler_params=vmem_mib(4),
        name="pack",
    )(gate, up)


def prep_kernel(
    x_ref, gain_ref, routes_ref, up_ref, down_ref,
    out_ref, slot_ref, wb_ref, normed_ref, sb_ref, sems,
):
    copies = [(up_ref.at[0, pl.ds(1024, 1024)], sb_ref.at[pl.ds(0, 1024)])] + [
        (down_ref.at[0, :, pl.ds(c * 256, 256)], sb_ref.at[pl.ds(1024 + c * 256, 256)])
        for c in range(8)
    ]
    copies = [pltpu.make_async_copy(s, d, sems.at[i]) for i, (s, d) in enumerate(copies)]
    for copy in copies:
        copy.start()

    def norm_rows(i, carry):
        rows = pl.ds(pl.multiple_of(i * 32, 32), 32)
        wide = x_ref[rows, :].astype(jnp.float32)
        scale = lax.rsqrt(jnp.mean(wide * wide, axis=1, keepdims=True) + NORM_EPS)
        normed_ref[rows, :] = (wide * scale * gain_ref[...]).astype(jnp.bfloat16)
        return carry

    lax.fori_loop(0, ROWS_B // 32, norm_rows, 0)
    for copy in copies:
        copy.wait()
    leave = pltpu.make_async_copy(sb_ref, wb_ref, sems.at[9])
    leave.start()

    first = routes_ref[0:1, :]
    second = routes_ref[1:2, :]
    expert = lax.broadcasted_iota(jnp.int32, (128, ROWS_B), 0)
    row = lax.broadcasted_iota(jnp.int32, (ROWS_B, ROWS_B), 0)
    col = lax.broadcasted_iota(jnp.int32, (ROWS_B, ROWS_B), 1)
    above = jnp.where(row < col, 1.0, 0.0).astype(jnp.bfloat16)
    named = jnp.where((first == expert) | (second == expert), 1.0, 0.0)
    rank = jnp.dot(named.astype(jnp.bfloat16), above, preferred_element_type=jnp.float32)
    rank_a = jnp.sum(jnp.where(first == expert, rank, 0.0), axis=0, keepdims=True)
    rank_b = jnp.sum(jnp.where(second == expert, rank, 0.0), axis=0, keepdims=True)
    slot_a = first * CAP + rank_a.astype(jnp.int32)
    slot_b = second * CAP + rank_b.astype(jnp.int32)
    both = jnp.where(expert == 0, slot_a, slot_b).astype(jnp.float32)
    slot_ref[...] = both.T.astype(jnp.int32)

    mark = jnp.where(named > 0.5, rank, -1.0).astype(jnp.bfloat16)
    spread = jnp.where(
        (lax.broadcasted_iota(jnp.int32, (ROWS_B, 128), 0) >> 3)
        == lax.broadcasted_iota(jnp.int32, (ROWS_B, 128), 1),
        1.0,
        0.0,
    ).astype(jnp.bfloat16)
    mark_rows = jnp.dot(spread, mark, preferred_element_type=jnp.float32)
    xi = lax.axis_index("x")
    yi = lax.axis_index("y")
    even = ((row >> 3) & 1) == 0
    wanted = jnp.where(even, xi, yi) * 8 + (row & 7)
    pick = jnp.where(mark_rows.astype(jnp.int32) == wanted, 1.0, 0.0).astype(jnp.bfloat16)
    from_y = jnp.dot(
        pick, normed_ref[:, pl.ds(pl.multiple_of(yi * 512, 512), 512)],
        preferred_element_type=jnp.float32,
    )
    from_x = jnp.dot(
        pick, normed_ref[:, pl.ds(pl.multiple_of(xi * 512, 512), 512)],
        preferred_element_type=jnp.float32,
    )
    even_row = ((lax.broadcasted_iota(jnp.int32, (ROWS_B, 512), 0) >> 3) & 1) == 0
    out_ref[...] = jnp.where(even_row, from_y, from_x).astype(jnp.bfloat16)
    leave.wait()


def prepare(expert_input, norm_gain, routes, up, down):
    return pl.pallas_call(
        prep_kernel,
        out_shape=(
            jax.ShapeDtypeStruct((ROWS_B, 512), jnp.bfloat16),
            jax.ShapeDtypeStruct((ROWS_B, 128), jnp.int32),
            jax.ShapeDtypeStruct((HALF_W, 256), jnp.bfloat16),
        ),
        in_specs=[VMEM, VMEM, VMEM, ANY, ANY],
        out_specs=(VMEM, VMEM, ANY),
        scratch_shapes=[
            pltpu.VMEM((ROWS_B, D), jnp.bfloat16),
            pltpu.VMEM((HALF_W, 256), jnp.bfloat16),
            pltpu.SemaphoreType.DMA((10,)),
        ],
        compiler_params=vmem_mib(16),
        name="prep",
    )(expert_input, norm_gain.reshape(1, D), routes.T, up, down)


def slice_hidden(x_ref, wa, wb):
    def part(m, ref, start):
        return jnp.dot(
            x_ref[m, pl.ds(0, ROWS_B), :], ref[pl.ds(start, 512), :],
            preferred_element_type=jnp.float32,
        )

    gate = part(0, wa, 0) + part(1, wa, 512) + part(2, wa, 1024) + part(3, wa, 1536)
    up = part(0, wa, 2048) + part(1, wa, 2560) + part(2, wb, 0) + part(3, wb, 512)
    return (gate / (1.0 + jnp.exp(-gate)) * up).astype(jnp.bfloat16)


def ffn_kernel(x_ref, *refs):
    weights, out_ref, acc_ref, bufs, sems = refs[:8], refs[8], refs[9], refs[10], refs[11]
    copies = [
        pltpu.make_async_copy(w, bufs.at[i], sems.at[i]) for i, w in enumerate(weights)
    ]
    for copy in copies:
        copy.start()
    core = lax.axis_index("co")
    for s in range(4):
        copies[2 * s].wait()
        copies[2 * s + 1].wait()
        wa, wb = bufs.at[2 * s], bufs.at[2 * s + 1]
        hidden = slice_hidden(x_ref, wa, wb)
        for c in range(8):
            cols = pl.ds(c * 256, 256)
            term = jnp.dot(
                hidden, wb[pl.ds(1024 + c * 256, 256), :], preferred_element_type=jnp.float32
            )
            total = term if s == 0 else acc_ref[:, cols] + term
            if s < 3:
                acc_ref[:, cols] = total
                continue
            for k in range(2):
                t = 2 * c + k
                place = jnp.where(core == 0, t, (t % 4) * 4 + t // 4)
                piece = total[:, k * 128 : (k + 1) * 128].astype(jnp.bfloat16)
                out_ref[place] = piece


def ffn(x, weights):
    return pl.pallas_call(
        ffn_kernel,
        out_shape=jax.ShapeDtypeStruct((16, ROWS_B, 128), jnp.bfloat16),
        in_specs=[VMEM] + [ANY] * 8,
        out_specs=VMEM,
        scratch_shapes=[
            pltpu.VMEM((ROWS_B, D), jnp.float32),
            pltpu.VMEM((8, HALF_W, 256), jnp.bfloat16),
            pltpu.SemaphoreType.DMA((8,)),
        ],
        compiler_params=vmem_mib(24),
        name="ffn",
    )(resident(x), *weights)


def combine_kernel(ret_ref, slot_ref, weight_ref, out_ref):
    place = lax.broadcasted_iota(jnp.int32, (ROWS_B, EXPERTS * CAP), 1)
    total = None
    for k in range(2):
        pick = jnp.where(place == slot_ref[:, k : k + 1], 1.0, 0.0).astype(jnp.bfloat16)
        rows = jnp.dot(pick, ret_ref[...], preferred_element_type=jnp.float32)
        term = rows * weight_ref[:, k : k + 1]
        total = term if total is None else total + term
    out_ref[...] = total.astype(jnp.bfloat16)


def combine(returned, slots, route_weights):
    return pl.pallas_call(
        combine_kernel,
        out_shape=jax.ShapeDtypeStruct((ROWS_B, 128), jnp.bfloat16),
        in_specs=[VMEM] * 3,
        out_specs=VMEM,
        compiler_params=vmem_mib(12),
        name="combine",
    )(resident(returned), slots, route_weights)


def project_kernel(own_ref, prev_ref, next_ref, far_ref, weight_ref, out_ref, a_ref, w_ref):
    core = lax.axis_index("co")
    line = jnp.where(core == 0, lax.axis_index("x"), lax.axis_index("y"))
    w_ref[...] = jnp.zeros_like(w_ref)
    for j, (ref, step) in enumerate(((own_ref, 0), (prev_ref, 3), (next_ref, 1), (far_ref, 2))):
        source = lax.rem(line + step, 4)
        for m in range(4):
            head = jnp.where(core == 0, m * 4 + source, source * 4 + m)
            at = (4 * j + m) * 128
            weight = weight_ref[pl.ds(pl.multiple_of(head * HEAD_DIM, HEAD_DIM), HEAD_DIM), :]
            w_ref[pl.ds(at, 64), pl.ds(0, 128)] = weight
            w_ref[pl.ds(at + 64, 64), pl.ds(128, 128)] = weight
            for q in range(4):
                a_ref[pl.ds(q * 64, 64), pl.ds(at, 128)] = ref[m, :, pl.ds(q * 128, 128)]
    both = jnp.dot(a_ref[...], w_ref[...], preferred_element_type=jnp.float32)
    out_ref[pl.ds(0, 256), :] = both[:, :128].astype(jnp.bfloat16)
    out_ref[pl.ds(256, 256), :] = both[:, 128:].astype(jnp.bfloat16)


def project(own, prev, nxt, far, out_weight):
    return pl.pallas_call(
        project_kernel,
        out_shape=jax.ShapeDtypeStruct((512, 128), jnp.bfloat16),
        in_specs=[VMEM] * 5,
        out_specs=VMEM,
        scratch_shapes=[
            pltpu.VMEM((256, 2048), jnp.bfloat16), pltpu.VMEM((2048, 256), jnp.bfloat16)
        ],
        compiler_params=vmem_mib(12),
        name="project",
    )(*(resident(a) for a in (own, prev, nxt, far, out_weight)))


def padded(block, axis, dim, width):
    count = lax.axis_size(axis)
    forward = [(i, i + 1) for i in range(count - 1)]
    backward = [(target, source) for source, target in forward]
    low = lax.ppermute(
        lax.slice_in_dim(block, block.shape[dim] - width, None, axis=dim), axis, forward
    )
    high = lax.ppermute(lax.slice_in_dim(block, 0, width, axis=dim), axis, backward)
    return jnp.concatenate([low, block, high], axis=dim)


def rotate(features, position_start):
    count = features.shape[0]
    half_dim = features.shape[-1] // 2
    inverse_freq = 1.0 / ROPE_BASE ** (
        jnp.arange(half_dim, dtype=jnp.float32) * 2.0 / features.shape[-1]
    )
    position = (jnp.arange(count, dtype=jnp.int32) + position_start).astype(jnp.float32)
    angles = position[:, None] * inverse_freq[None, :]
    cosine = jnp.cos(angles)[:, None, :]
    sine_part = jnp.sin(angles)[:, None, :]
    lower_half = features[..., :half_dim]
    upper_half = features[..., half_dim:]
    return jnp.concatenate(
        [
            lower_half * cosine - upper_half * sine_part,
            upper_half * cosine + lower_half * sine_part,
        ],
        axis=-1,
    )


def attend(query_proj, key_proj, value_proj, sink_logit):
    row_count = query_proj.shape[0]
    local_heads = query_proj.shape[1] // HEAD_DIM
    per_kv = HEADS // KV_HEADS
    kv_local = max(1, local_heads // per_kv)
    group_size = local_heads // kv_local
    tp_index = lax.axis_index(TP)
    offset = lax.axis_index(EP) * row_count
    seq_total = row_count * lax.axis_size(EP)
    first_kv = tp_index * local_heads // per_kv
    own_keys = lax.dynamic_slice_in_dim(key_proj, first_kv * HEAD_DIM, kv_local * HEAD_DIM, 1)
    own_values = lax.dynamic_slice_in_dim(value_proj, first_kv * HEAD_DIM, kv_local * HEAD_DIM, 1)
    rot_q = rotate(
        query_proj.reshape(row_count, local_heads, HEAD_DIM).astype(jnp.float32), offset
    ).astype(jnp.bfloat16)
    rot_k = rotate(
        own_keys.reshape(row_count, kv_local, HEAD_DIM).astype(jnp.float32), offset
    ).astype(jnp.bfloat16)
    stacked = jnp.stack([rot_k, own_values.reshape(row_count, kv_local, HEAD_DIM)])
    extended = padded(stacked, EP, 1, HALF_WIN)
    own_sink = sink_logit.reshape(kv_local, group_size)
    block_rows = row_count
    key_rows = block_rows + 2 * HALF_WIN
    key_offset = jnp.arange(key_rows, dtype=jnp.int32) - HALF_WIN
    key_gap = key_offset[None, :] - jnp.arange(block_rows, dtype=jnp.int32)[:, None]
    query_block = rot_q.reshape(block_rows, kv_local, group_size, HEAD_DIM)
    scores = jnp.einsum(
        "qngd,knd->ngqk", query_block, extended[0], preferred_element_type=jnp.float32
    ) * HEAD_DIM ** (-0.5)
    global_key = offset + key_offset
    allowed = (
        (jnp.abs(key_gap) <= HALF_WIN)
        & (global_key >= 0)[None, :]
        & (global_key < seq_total)[None, :]
    )
    scores = jnp.where(allowed[None, None], scores, NEG_BIG)
    row_peak = jnp.maximum(jnp.max(scores, axis=-1), own_sink[:, :, None])
    lifted = jnp.exp(scores - row_peak[..., None])
    norm_total = jnp.sum(lifted, axis=-1) + jnp.exp(own_sink[:, :, None] - row_peak)
    probs = (lifted / norm_total[..., None]).astype(jnp.bfloat16)
    weighted = jnp.einsum("ngqk,knd->qngd", probs, extended[1], preferred_element_type=jnp.float32)
    return weighted.astype(jnp.bfloat16).reshape(block_rows, local_heads * HEAD_DIM)


def local(
    query_proj,
    key_proj,
    value_proj,
    sink_logit,
    out_weight,
    expert_input,
    norm_gain,
    routes,
    route_weights,
    gate_weight,
    up_weight,
    down_weight,
):
    wa = pack(gate_weight, up_weight)
    prev_a = line_shift(wa, 1)
    next_a = line_shift(wa, -1)
    outgoing, slots, wb = prepare(
        expert_input, norm_gain, routes, up_weight, down_weight
    )
    next_b = line_shift(wb, -1)
    prev_b = line_shift(wb, 1)
    arrived = lax.all_to_all(outgoing, EP, 0, 0, tiled=True)
    far_a = line_shift(prev_a, 1)
    far_b = line_shift(next_b, -1)

    attended = attend(query_proj, key_proj, value_proj, sink_logit)
    packed = jnp.concatenate([attended[:256], attended[256:]], axis=1)
    packed = jnp.concatenate([packed[q * 64 : (q + 1) * 64] for q in range(4)], axis=1)

    payload = jnp.concatenate([arrived, packed], axis=0)
    rows = lax.all_to_all(
        jnp.broadcast_to(payload[None], (4, *payload.shape)),
        PLANE, 0, 0, tiled=True, axis_index_groups=LINE_M,
    )
    partial = ffn(rows, (wa, wb, prev_a, prev_b, next_a, next_b, far_a, far_b))
    parts = lax.all_to_all(partial, PLANE, 0, 0, tiled=True, axis_index_groups=WHOLE)
    parts = parts.reshape(4, 4, 256, 128)
    result = jnp.sum(parts.astype(jnp.float32), axis=0).astype(jnp.bfloat16)
    result = jnp.moveaxis(result.reshape(4, EXPERTS, 8, 128), 0, 1)
    result = result.reshape(EXPERTS, CAP, 128)
    returned = lax.all_to_all(result, EP, 0, 0, tiled=True)
    expert_out = combine(returned.reshape(EXPERTS * CAP, 128), slots, route_weights)

    heads = rows[:, 256:]
    around = [line_shift(heads, step) for step in (1, -1, 2)]
    mixer_out = project(heads, *around, out_weight)
    return (mixer_out, expert_out)


def solution(mesh):
    finer = Mesh(mesh.devices.reshape(16, 2, 4, 4), ("z", "co", "y", "x"))
    in_specs = (
        P(EP, TP),
        P(EP, None),
        P(EP, None),
        P(TP),
        P(None, TP),
        P(EP, None),
        P(),
        P(EP, None),
        P(EP, None),
        P(EP, None, TP),
        P(EP, None, TP),
        P(EP, TP, None),
    )
    out_specs = (P(EP, TP), P(EP, TP))
    return jax.shard_map(local, mesh=finer, in_specs=in_specs, out_specs=out_specs, check_vma=False)
```

```python
import jax
import jax.numpy as jnp
from jax import lax
from jax.experimental import pallas as pl
from jax.experimental.pallas import tpu as pltpu
from jax.sharding import Mesh
from jax.sharding import PartitionSpec as P


D = 2048
HEAD_DIM = 64
HALF_WIN = 128
ROWS_B = 256
EXPERTS = 32
CAP = 32
EP = ("z", "co")
TP = ("y", "x")
PLANE = ("co", "y", "x")

NORM_EPS = 1e-06
ROPE_BASE = 10000.0
NEG_BIG = -1e30

LINE_L = [[y * 4 + x for x in range(4)] for y in range(4)] + [
    [16 + y * 4 + x for y in range(4)] for x in range(4)
]
LINE_M = [[y * 4 + x for y in range(4)] for x in range(4)] + [
    [16 + y * 4 + x for x in range(4)] for y in range(4)
]
WHOLE = [list(range(16)), [16 + (p % 4) * 4 + p // 4 for p in range(16)]]


ANY = pl.BlockSpec(memory_space=pl.ANY)
VMEM = pl.BlockSpec(memory_space=pltpu.VMEM)
HALF_W = 3072


def resident(x):
    return pltpu.with_memory_space_constraint(x, pltpu.VMEM)


def vmem_mib(count):
    return pltpu.CompilerParams(vmem_limit_bytes=count << 20)


def line_shift(x, step):
    pairs = [(line[i], line[(i + step) % 4]) for line in LINE_L for i in range(4)]
    return lax.ppermute(x, PLANE, pairs)


def pack_kernel(pieces, *refs):
    sources, out_ref, stage_ref, sems = refs[:-3], refs[-3], refs[-2], refs[-1]
    copies, leave = [], []
    for i, (which, rows, cols, at) in enumerate(pieces):
        source = sources[which].at[0, pl.ds(*rows), pl.ds(*cols)]
        part = pl.ds(at, rows[1])
        copies.append(pltpu.make_async_copy(source, stage_ref.at[part], sems.at[0, i]))
        leave.append(
            pltpu.make_async_copy(stage_ref.at[part], out_ref.at[part], sems.at[1, i])
        )
    for copy in copies:
        copy.start()
    for come, go in zip(copies, leave):
        come.wait()
        go.start()
    for go in leave:
        go.wait()


def pack(pieces, *sources):
    def body(*refs):
        pack_kernel(pieces, *refs)

    return pl.pallas_call(
        body,
        out_shape=jax.ShapeDtypeStruct((HALF_W, 256), jnp.bfloat16),
        in_specs=[ANY] * len(sources),
        out_specs=ANY,
        scratch_shapes=[
            pltpu.VMEM((HALF_W, 256), jnp.bfloat16),
            pltpu.SemaphoreType.DMA((2, len(pieces))),
        ],
        compiler_params=vmem_mib(4),
        name="pack",
    )(*sources)


PIECES_A = ((0, (0, 2048), (0, 256), 0), (1, (0, 1024), (0, 256), 2048))
PIECES_B = ((0, (1024, 1024), (0, 256), 0),) + tuple(
    (1, (0, 256), (c * 256, 256), 1024 + c * 256) for c in range(8)
)


def prep_kernel(x_ref, gain_ref, routes_ref, out_ref, slot_ref, normed_ref):
    def norm_rows(i, carry):
        rows = pl.ds(pl.multiple_of(i * 32, 32), 32)
        wide = x_ref[rows, :].astype(jnp.float32)
        scale = lax.rsqrt(jnp.mean(wide * wide, axis=1, keepdims=True) + NORM_EPS)
        normed_ref[rows, :] = (wide * scale * gain_ref[...]).astype(jnp.bfloat16)
        return carry

    lax.fori_loop(0, ROWS_B // 32, norm_rows, 0)

    first = routes_ref[0:1, :]
    second = routes_ref[1:2, :]
    expert = lax.broadcasted_iota(jnp.int32, (128, ROWS_B), 0)
    row = lax.broadcasted_iota(jnp.int32, (ROWS_B, ROWS_B), 0)
    col = lax.broadcasted_iota(jnp.int32, (ROWS_B, ROWS_B), 1)
    above = jnp.where(row < col, 1.0, 0.0).astype(jnp.bfloat16)
    named = jnp.where((first == expert) | (second == expert), 1.0, 0.0)
    rank = jnp.dot(named.astype(jnp.bfloat16), above, preferred_element_type=jnp.float32)
    rank_a = jnp.sum(jnp.where(first == expert, rank, 0.0), axis=0, keepdims=True)
    rank_b = jnp.sum(jnp.where(second == expert, rank, 0.0), axis=0, keepdims=True)
    slot_a = first * CAP + rank_a.astype(jnp.int32)
    slot_b = second * CAP + rank_b.astype(jnp.int32)
    both = jnp.where(expert == 0, slot_a, slot_b).astype(jnp.float32)
    slot_ref[...] = both.T.astype(jnp.int32)

    mark = jnp.where(named > 0.5, rank, -1.0).astype(jnp.bfloat16)
    spread = jnp.where(
        (lax.broadcasted_iota(jnp.int32, (ROWS_B, 128), 0) >> 3)
        == lax.broadcasted_iota(jnp.int32, (ROWS_B, 128), 1),
        1.0,
        0.0,
    ).astype(jnp.bfloat16)
    mark_rows = jnp.dot(spread, mark, preferred_element_type=jnp.float32)
    xi = lax.axis_index("x")
    yi = lax.axis_index("y")
    even = ((row >> 3) & 1) == 0
    wanted = jnp.where(even, xi, yi) * 8 + (row & 7)
    pick = jnp.where(mark_rows.astype(jnp.int32) == wanted, 1.0, 0.0).astype(jnp.bfloat16)
    from_y = jnp.dot(
        pick, normed_ref[:, pl.ds(pl.multiple_of(yi * 512, 512), 512)],
        preferred_element_type=jnp.float32,
    )
    from_x = jnp.dot(
        pick, normed_ref[:, pl.ds(pl.multiple_of(xi * 512, 512), 512)],
        preferred_element_type=jnp.float32,
    )
    even_row = ((lax.broadcasted_iota(jnp.int32, (ROWS_B, 512), 0) >> 3) & 1) == 0
    out_ref[...] = jnp.where(even_row, from_y, from_x).astype(jnp.bfloat16)


def prepare(expert_input, norm_gain, routes):
    return pl.pallas_call(
        prep_kernel,
        out_shape=(
            jax.ShapeDtypeStruct((ROWS_B, 512), jnp.bfloat16),
            jax.ShapeDtypeStruct((ROWS_B, 128), jnp.int32),
        ),
        in_specs=[VMEM] * 3,
        out_specs=(VMEM, VMEM),
        scratch_shapes=[pltpu.VMEM((ROWS_B, D), jnp.bfloat16)],
        compiler_params=vmem_mib(16),
        name="prep",
    )(expert_input, norm_gain.reshape(1, D), routes.T)


def slice_hidden(x_ref, wa, wb):
    def part(m, ref, start):
        return jnp.dot(
            x_ref[m, pl.ds(0, ROWS_B), :], ref[pl.ds(start, 512), :],
            preferred_element_type=jnp.float32,
        )

    gate = part(0, wa, 0) + part(1, wa, 512) + part(2, wa, 1024) + part(3, wa, 1536)
    up = part(0, wa, 2048) + part(1, wa, 2560) + part(2, wb, 0) + part(3, wb, 512)
    return (gate / (1.0 + jnp.exp(-gate)) * up).astype(jnp.bfloat16)


def ffn_kernel(x_ref, *refs):
    weights, out_ref, acc_ref, bufs, sems, piece_ref, out_sems = refs[:8], *refs[8:]
    leave = []
    copies = [
        pltpu.make_async_copy(w, bufs.at[i], sems.at[i]) for i, w in enumerate(weights)
    ]
    for copy in copies:
        copy.start()
    core = lax.axis_index("co")
    for s in range(4):
        copies[2 * s].wait()
        copies[2 * s + 1].wait()
        wa, wb = bufs.at[2 * s], bufs.at[2 * s + 1]
        hidden = slice_hidden(x_ref, wa, wb)
        for c in range(8):
            cols = pl.ds(c * 256, 256)
            term = jnp.dot(
                hidden, wb[pl.ds(1024 + c * 256, 256), :], preferred_element_type=jnp.float32
            )
            total = term if s == 0 else acc_ref[:, cols] + term
            if s < 3:
                acc_ref[:, cols] = total
                continue
            for k in range(2):
                t = 2 * c + k
                place = jnp.where(core == 0, t, (t % 4) * 4 + t // 4)
                piece = total[:, k * 128 : (k + 1) * 128].astype(jnp.bfloat16)
                piece_ref[t] = piece
                leave.append(
                    pltpu.make_async_copy(piece_ref.at[t], out_ref.at[place], out_sems.at[t])
                )
                leave[-1].start()
    for copy in leave:
        copy.wait()


def ffn(x, weights):
    return pl.pallas_call(
        ffn_kernel,
        out_shape=pltpu.HBM((16, ROWS_B, 128), jnp.bfloat16),
        in_specs=[VMEM] + [ANY] * 8,
        out_specs=pl.BlockSpec(memory_space=pltpu.HBM),
        scratch_shapes=[
            pltpu.VMEM((ROWS_B, D), jnp.float32),
            pltpu.VMEM((8, HALF_W, 256), jnp.bfloat16),
            pltpu.SemaphoreType.DMA((8,)),
            pltpu.VMEM((16, ROWS_B, 128), jnp.bfloat16),
            pltpu.SemaphoreType.DMA((16,)),
        ],
        compiler_params=vmem_mib(24),
        name="ffn",
    )(resident(x), *weights)


def combine_kernel(ret_ref, slot_ref, weight_ref, out_ref):
    place = lax.broadcasted_iota(jnp.int32, (ROWS_B, EXPERTS * CAP), 1)
    total = None
    for k in range(2):
        pick = jnp.where(place == slot_ref[:, k : k + 1], 1.0, 0.0).astype(jnp.bfloat16)
        rows = jnp.dot(pick, ret_ref[...], preferred_element_type=jnp.float32)
        term = rows * weight_ref[:, k : k + 1]
        total = term if total is None else total + term
    out_ref[...] = total.astype(jnp.bfloat16)


def combine(returned, slots, route_weights):
    return pl.pallas_call(
        combine_kernel,
        out_shape=jax.ShapeDtypeStruct((ROWS_B, 128), jnp.bfloat16),
        in_specs=[VMEM] * 3,
        out_specs=VMEM,
        compiler_params=vmem_mib(12),
        name="combine",
    )(resident(returned), slots, route_weights)


def project_kernel(own_ref, prev_ref, next_ref, far_ref, weight_ref, out_ref, a_ref):
    core = lax.axis_index("co")
    line = jnp.where(core == 0, lax.axis_index("x"), lax.axis_index("y"))
    for ref, step in ((own_ref, 0), (prev_ref, 3), (next_ref, 1), (far_ref, 2)):
        source = lax.rem(line + step, 4)
        for m in range(4):
            head = jnp.where(core == 0, m * 4 + source, source * 4 + m)
            a_ref[pl.ds(pl.multiple_of(head * HEAD_DIM, HEAD_DIM), HEAD_DIM), :] = ref[m]
    turned = weight_ref[...].astype(jnp.float32).T.astype(jnp.bfloat16)
    out = jnp.dot(turned, a_ref[...], preferred_element_type=jnp.float32)
    out_ref[...] = out.T.astype(jnp.bfloat16)


def project(own, prev, nxt, far, out_weight):
    return pl.pallas_call(
        project_kernel,
        out_shape=jax.ShapeDtypeStruct((512, 128), jnp.bfloat16),
        in_specs=[VMEM] * 5,
        out_specs=VMEM,
        scratch_shapes=[pltpu.VMEM((1024, 512), jnp.bfloat16)],
        compiler_params=vmem_mib(12),
        name="project",
    )(*(resident(a) for a in (own, prev, nxt, far, out_weight)))


def attend_kernel(q_ref, kv_ref, low_ref, high_ref, cos_ref, sin_ref, sink_ref, out_ref,
                  k_scr, vt_scr):
    half = HEAD_DIM // 2

    def turn(x, rows):
        wide = x.astype(jnp.float32)
        swapped = jnp.concatenate([wide[:, half:], wide[:, :half]], axis=1)
        return (wide * cos_ref[rows, :] + swapped * sin_ref[rows, :]).astype(jnp.bfloat16)

    spans = ((low_ref, 0, HALF_WIN), (kv_ref, HALF_WIN, 512), (high_ref, 512 + HALF_WIN, HALF_WIN))
    for ref, at, count in spans:
        rows = pl.ds(at, count)
        k_scr[rows, :] = turn(ref[0], rows)
        value = ref[1].astype(jnp.float32)
        vt_scr[:, rows] = jnp.concatenate([value, value], axis=1).T.astype(jnp.bfloat16)
    start = (lax.axis_index("z") * 2 + lax.axis_index("co")) * 512
    key_at = lax.broadcasted_iota(jnp.int32, (384, 128), 0) - HALF_WIN
    gap = key_at - lax.broadcasted_iota(jnp.int32, (384, 128), 1)
    sink = sink_ref[0]
    for j in range(4):
        query = turn(q_ref[pl.ds(j * 128, 128), :], pl.ds(HALF_WIN + j * 128, 128))
        scores = lax.dot_general(
            k_scr[pl.ds(j * 128, 384), :], query, (((1,), (1,)), ((), ())),
            preferred_element_type=jnp.float32,
        ) * HEAD_DIM ** (-0.5)
        key = key_at + (start + j * 128)
        allowed = (jnp.abs(gap) <= HALF_WIN) & (key >= 0) & (key < 16384)
        scores = jnp.where(allowed, scores, NEG_BIG)
        peak = jnp.maximum(jnp.max(scores, axis=0, keepdims=True), sink)
        lifted = jnp.exp(scores - peak)
        total = jnp.sum(lifted, axis=0, keepdims=True) + jnp.exp(sink - peak)
        probs = (lifted / total).astype(jnp.bfloat16)
        mixed = jnp.dot(
            vt_scr[pl.ds(0, HEAD_DIM), pl.ds(j * 128, 384)], probs,
            preferred_element_type=jnp.float32,
        )
        out_ref[:, pl.ds(j * 128, 128)] = mixed.astype(jnp.bfloat16)


def attend(query_proj, key_proj, value_proj, sink_logit):
    kv_at = lax.axis_index("y") * HEAD_DIM
    own = jnp.stack(
        [lax.dynamic_slice_in_dim(a, kv_at, HEAD_DIM, 1) for a in (key_proj, value_proj)]
    )
    count = lax.axis_size(EP)
    forward = [(i, i + 1) for i in range(count - 1)]
    backward = [(target, source) for source, target in forward]
    low = lax.ppermute(own[:, 512 - HALF_WIN :], EP, forward)
    high = lax.ppermute(own[:, :HALF_WIN], EP, backward)
    offset = lax.axis_index(EP) * 512 - HALF_WIN
    half = HEAD_DIM // 2
    channel = jnp.arange(HEAD_DIM, dtype=jnp.int32)
    inverse_freq = 1.0 / ROPE_BASE ** ((channel % half).astype(jnp.float32) * 2.0 / HEAD_DIM)
    position = (jnp.arange(512 + 2 * HALF_WIN, dtype=jnp.int32) + offset).astype(jnp.float32)
    angles = position[:, None] * inverse_freq[None, :]
    cosine = jnp.cos(angles)
    sine = jnp.where(channel < half, -1.0, 1.0)[None, :] * jnp.sin(angles)
    return pl.pallas_call(
        attend_kernel,
        out_shape=jax.ShapeDtypeStruct((HEAD_DIM, 512), jnp.bfloat16),
        in_specs=[VMEM] * 6 + [pl.BlockSpec(memory_space=pltpu.SMEM)],
        out_specs=VMEM,
        scratch_shapes=[
            pltpu.VMEM((768, HEAD_DIM), jnp.bfloat16), pltpu.VMEM((128, 768), jnp.bfloat16)
        ],
        compiler_params=vmem_mib(12),
        name="attend",
    )(*(resident(a) for a in (query_proj, own, low, high, cosine, sine)), sink_logit)


def local(
    query_proj,
    key_proj,
    value_proj,
    sink_logit,
    out_weight,
    expert_input,
    norm_gain,
    routes,
    route_weights,
    gate_weight,
    up_weight,
    down_weight,
):
    wa = pack(PIECES_A, gate_weight, up_weight)
    prev_a = line_shift(wa, 1)
    wb = pack(PIECES_B, up_weight, down_weight)
    next_b = line_shift(wb, -1)
    outgoing, slots = prepare(expert_input, norm_gain, routes)
    next_a = line_shift(wa, -1)
    prev_b = line_shift(wb, 1)
    arrived = lax.all_to_all(outgoing, EP, 0, 0, tiled=True)
    far_a = line_shift(prev_a, 1)
    far_b = line_shift(next_b, -1)

    attended = attend(query_proj, key_proj, value_proj, sink_logit)

    payload = jnp.concatenate([arrived, attended], axis=0)
    rows = lax.all_to_all(
        jnp.broadcast_to(payload[None], (4, *payload.shape)),
        PLANE, 0, 0, tiled=True, axis_index_groups=LINE_M,
    )
    partial = ffn(rows, (wa, wb, prev_a, prev_b, next_a, next_b, far_a, far_b))
    parts = lax.all_to_all(partial, PLANE, 0, 0, tiled=True, axis_index_groups=WHOLE)
    parts = parts.reshape(4, 4, 256, 128)
    result = jnp.sum(parts.astype(jnp.float32), axis=0).astype(jnp.bfloat16)
    result = jnp.moveaxis(result.reshape(4, EXPERTS, 8, 128), 0, 1)
    result = result.reshape(EXPERTS, CAP, 128)
    returned = lax.all_to_all(result, EP, 0, 0, tiled=True)
    expert_out = combine(returned.reshape(EXPERTS * CAP, 128), slots, route_weights)

    heads = rows[:, 256:]
    around = [line_shift(heads, step) for step in (1, -1, 2)]
    mixer_out = project(heads, *around, out_weight)
    return (mixer_out, expert_out)


def solution(mesh):
    finer = Mesh(mesh.devices.reshape(16, 2, 4, 4), ("z", "co", "y", "x"))
    in_specs = (
        P(EP, TP),
        P(EP, None),
        P(EP, None),
        P(TP),
        P(None, TP),
        P(EP, None),
        P(),
        P(EP, None),
        P(EP, None),
        P(EP, None, TP),
        P(EP, None, TP),
        P(EP, TP, None),
    )
    out_specs = (P(EP, TP), P(EP, TP))
    return jax.shard_map(local, mesh=finer, in_specs=in_specs, out_specs=out_specs, check_vma=False)
```

```python
import jax
import jax.numpy as jnp
from jax import lax
from jax.experimental import pallas as pl
from jax.experimental.pallas import tpu as pltpu
from jax.sharding import Mesh
from jax.sharding import PartitionSpec as P


D = 2048
HEAD_DIM = 64
HALF_WIN = 128
ROWS_B = 256
EXPERTS = 32
CAP = 32
EP = ("z", "co")
TP = ("y", "x")
PLANE = ("co", "y", "x")

NORM_EPS = 1e-06
ROPE_BASE = 10000.0
NEG_BIG = -1e30

LINE_L = [[y * 4 + x for x in range(4)] for y in range(4)] + [
    [16 + y * 4 + x for y in range(4)] for x in range(4)
]
LINE_M = [[y * 4 + x for y in range(4)] for x in range(4)] + [
    [16 + y * 4 + x for x in range(4)] for y in range(4)
]
WHOLE = [list(range(16)), [16 + (p % 4) * 4 + p // 4 for p in range(16)]]


ANY = pl.BlockSpec(memory_space=pl.ANY)
VMEM = pl.BlockSpec(memory_space=pltpu.VMEM)
IN_HBM = pl.BlockSpec(memory_space=pltpu.HBM)
HALF_W = 3072


def resident(x):
    return pltpu.with_memory_space_constraint(x, pltpu.VMEM)


def in_hbm(x):
    return pltpu.with_memory_space_constraint(x, pltpu.HBM)


def vmem_mib(count):
    return pltpu.CompilerParams(vmem_limit_bytes=count << 20)


def line_shift(x, step):
    pairs = [(line[i], line[(i + step) % 4]) for line in LINE_L for i in range(4)]
    return lax.ppermute(x, PLANE, pairs)


def pack(pieces, *sources):
    def body(*refs):
        inputs, out_ref, sems = refs[:-2], refs[-2], refs[-1]
        copies = [
            pltpu.make_async_copy(
                inputs[which].at[0, pl.ds(*rows), pl.ds(*cols)],
                out_ref.at[pl.ds(at, rows[1])],
                sems.at[i],
            )
            for i, (which, rows, cols, at) in enumerate(pieces)
        ]
        for copy in copies:
            copy.start()
        for copy in copies:
            copy.wait()

    return pl.pallas_call(
        body,
        out_shape=pltpu.VMEM((HALF_W, 256), jnp.bfloat16),
        in_specs=[IN_HBM] * len(sources),
        out_specs=VMEM,
        scratch_shapes=[pltpu.SemaphoreType.DMA((len(pieces),))],
        compiler_params=vmem_mib(4),
        name="pack",
    )(*(in_hbm(a) for a in sources))


PIECES_A = ((0, (0, 2048), (0, 256), 0), (1, (0, 1024), (0, 256), 2048))
PIECES_B = ((0, (1024, 1024), (0, 256), 0),) + tuple(
    (1, (0, 256), (c * 256, 256), 1024 + c * 256) for c in range(8)
)


def prep_kernel(x_ref, gain_ref, routes_ref, out_ref, slot_ref, normed_ref):
    def norm_rows(i, carry):
        rows = pl.ds(pl.multiple_of(i * 32, 32), 32)
        wide = x_ref[rows, :].astype(jnp.float32)
        scale = lax.rsqrt(jnp.mean(wide * wide, axis=1, keepdims=True) + NORM_EPS)
        normed_ref[rows, :] = (wide * scale * gain_ref[...]).astype(jnp.bfloat16)
        return carry

    lax.fori_loop(0, ROWS_B // 32, norm_rows, 0)

    first = routes_ref[0:1, :]
    second = routes_ref[1:2, :]
    expert = lax.broadcasted_iota(jnp.int32, (128, ROWS_B), 0)
    row = lax.broadcasted_iota(jnp.int32, (ROWS_B, ROWS_B), 0)
    col = lax.broadcasted_iota(jnp.int32, (ROWS_B, ROWS_B), 1)
    above = jnp.where(row < col, 1.0, 0.0).astype(jnp.bfloat16)
    named = jnp.where((first == expert) | (second == expert), 1.0, 0.0)
    rank = jnp.dot(named.astype(jnp.bfloat16), above, preferred_element_type=jnp.float32)
    rank_a = jnp.sum(jnp.where(first == expert, rank, 0.0), axis=0, keepdims=True)
    rank_b = jnp.sum(jnp.where(second == expert, rank, 0.0), axis=0, keepdims=True)
    slot_a = first * CAP + rank_a.astype(jnp.int32)
    slot_b = second * CAP + rank_b.astype(jnp.int32)
    both = jnp.where(expert == 0, slot_a, slot_b).astype(jnp.float32)
    slot_ref[...] = both.T.astype(jnp.int32)

    mark = jnp.where(named > 0.5, rank, -1.0).astype(jnp.bfloat16)
    spread = jnp.where(
        (lax.broadcasted_iota(jnp.int32, (ROWS_B, 128), 0) >> 3)
        == lax.broadcasted_iota(jnp.int32, (ROWS_B, 128), 1),
        1.0,
        0.0,
    ).astype(jnp.bfloat16)
    mark_rows = jnp.dot(spread, mark, preferred_element_type=jnp.float32)
    xi = lax.axis_index("x")
    yi = lax.axis_index("y")
    even = ((row >> 3) & 1) == 0
    wanted = jnp.where(even, xi, yi) * 8 + (row & 7)
    pick = jnp.where(mark_rows.astype(jnp.int32) == wanted, 1.0, 0.0).astype(jnp.bfloat16)
    from_y = jnp.dot(
        pick, normed_ref[:, pl.ds(pl.multiple_of(yi * 512, 512), 512)],
        preferred_element_type=jnp.float32,
    )
    from_x = jnp.dot(
        pick, normed_ref[:, pl.ds(pl.multiple_of(xi * 512, 512), 512)],
        preferred_element_type=jnp.float32,
    )
    even_row = ((lax.broadcasted_iota(jnp.int32, (ROWS_B, 512), 0) >> 3) & 1) == 0
    out_ref[...] = jnp.where(even_row, from_y, from_x).astype(jnp.bfloat16)


def prepare(expert_input, norm_gain, routes):
    return pl.pallas_call(
        prep_kernel,
        out_shape=(
            jax.ShapeDtypeStruct((ROWS_B, 512), jnp.bfloat16),
            jax.ShapeDtypeStruct((ROWS_B, 128), jnp.int32),
        ),
        in_specs=[VMEM] * 3,
        out_specs=(VMEM, VMEM),
        scratch_shapes=[pltpu.VMEM((ROWS_B, D), jnp.bfloat16)],
        compiler_params=vmem_mib(16),
        name="prep",
    )(expert_input, norm_gain.reshape(1, D), routes.T)


def slice_hidden(x_ref, wa, wb):
    def part(m, ref, start):
        return jnp.dot(
            x_ref[m, pl.ds(0, ROWS_B), :], ref[pl.ds(start, 512), :],
            preferred_element_type=jnp.float32,
        )

    gate = part(0, wa, 0) + part(1, wa, 512) + part(2, wa, 1024) + part(3, wa, 1536)
    up = part(0, wa, 2048) + part(1, wa, 2560) + part(2, wb, 0) + part(3, wb, 512)
    return (gate / (1.0 + jnp.exp(-gate)) * up).astype(jnp.bfloat16)


def ffn_kernel(x_ref, *refs):
    weights, out_ref, acc_ref, bufs, sems, piece_ref, out_sems = refs[:8], *refs[8:]
    copies = [pltpu.make_async_copy(w, bufs.at[i], sems.at[i]) for i, w in enumerate(weights)]
    for copy in copies:
        copy.start()
    core = lax.axis_index("co")
    leave = []
    for s in range(4):
        copies[2 * s].wait()
        copies[2 * s + 1].wait()
        wa, wb = bufs.at[2 * s], bufs.at[2 * s + 1]
        hidden = slice_hidden(x_ref, wa, wb)
        for c in range(8):
            cols = pl.ds(c * 256, 256)
            term = jnp.dot(
                hidden, wb[pl.ds(1024 + c * 256, 256), :], preferred_element_type=jnp.float32
            )
            total = term if s == 0 else acc_ref[:, cols] + term
            if s < 3:
                acc_ref[:, cols] = total
                continue
            for k in range(2):
                t = 2 * c + k
                place = jnp.where(core == 0, t, (t % 4) * 4 + t // 4)
                piece_ref[t] = total[:, k * 128 : (k + 1) * 128].astype(jnp.bfloat16)
                leave.append(
                    pltpu.make_async_copy(piece_ref.at[t], out_ref.at[place], out_sems.at[t])
                )
                leave[-1].start()
    for copy in leave:
        copy.wait()


def ffn(x, weights):
    return pl.pallas_call(
        ffn_kernel,
        out_shape=pltpu.HBM((16, ROWS_B, 128), jnp.bfloat16),
        in_specs=[VMEM] + [ANY] * 8,
        out_specs=IN_HBM,
        scratch_shapes=[
            pltpu.VMEM((ROWS_B, D), jnp.float32),
            pltpu.VMEM((8, HALF_W, 256), jnp.bfloat16),
            pltpu.SemaphoreType.DMA((8,)),
            pltpu.VMEM((16, ROWS_B, 128), jnp.bfloat16),
            pltpu.SemaphoreType.DMA((16,)),
        ],
        compiler_params=vmem_mib(24),
        name="ffn",
    )(resident(x), *weights)


def total_kernel(parts_ref, out_ref):
    for l in range(4):
        rows = sum(parts_ref[4 * m + l].astype(jnp.float32) for m in range(4))
        out_ref[:, l] = rows.astype(jnp.bfloat16).reshape(EXPERTS, 8, 128)


def total(parts):
    return pl.pallas_call(
        total_kernel,
        out_shape=jax.ShapeDtypeStruct((EXPERTS, 4, 8, 128), jnp.bfloat16),
        in_specs=[VMEM],
        out_specs=VMEM,
        compiler_params=vmem_mib(8),
        name="total",
    )(resident(parts))


def combine_kernel(ret_ref, slot_ref, weight_ref, out_ref):
    place = lax.broadcasted_iota(jnp.int32, (ROWS_B, EXPERTS * CAP), 1)
    total = None
    for k in range(2):
        pick = jnp.where(place == slot_ref[:, k : k + 1], 1.0, 0.0).astype(jnp.bfloat16)
        rows = jnp.dot(pick, ret_ref[...], preferred_element_type=jnp.float32)
        term = rows * weight_ref[:, k : k + 1]
        total = term if total is None else total + term
    out_ref[...] = total.astype(jnp.bfloat16)


def combine(returned, slots, route_weights):
    return pl.pallas_call(
        combine_kernel,
        out_shape=jax.ShapeDtypeStruct((ROWS_B, 128), jnp.bfloat16),
        in_specs=[VMEM] * 3,
        out_specs=VMEM,
        compiler_params=vmem_mib(12),
        name="combine",
    )(resident(returned), slots, route_weights)


def project_kernel(own_ref, prev_ref, next_ref, far_ref, weight_ref, out_ref, a_ref):
    core = lax.axis_index("co")
    line = jnp.where(core == 0, lax.axis_index("x"), lax.axis_index("y"))
    for ref, step in ((own_ref, 0), (prev_ref, 3), (next_ref, 1), (far_ref, 2)):
        source = lax.rem(line + step, 4)
        for m in range(4):
            head = jnp.where(core == 0, m * 4 + source, source * 4 + m)
            a_ref[pl.ds(pl.multiple_of(head * HEAD_DIM, HEAD_DIM), HEAD_DIM), :] = ref[m]
    turned = weight_ref[...].astype(jnp.float32).T.astype(jnp.bfloat16)
    out = jnp.dot(turned, a_ref[...], preferred_element_type=jnp.float32)
    out_ref[...] = out.T.astype(jnp.bfloat16)


def project(own, prev, nxt, far, out_weight):
    return pl.pallas_call(
        project_kernel,
        out_shape=jax.ShapeDtypeStruct((512, 128), jnp.bfloat16),
        in_specs=[VMEM] * 5,
        out_specs=VMEM,
        scratch_shapes=[pltpu.VMEM((1024, 512), jnp.bfloat16)],
        compiler_params=vmem_mib(12),
        name="project",
    )(*(resident(a) for a in (own, prev, nxt, far, out_weight)))


def attend_kernel(q_ref, kv_ref, low_ref, high_ref, cos_ref, sin_ref, sink_ref, out_ref,
                  k_scr, vt_scr):
    half = HEAD_DIM // 2

    def turn(x, rows):
        wide = x.astype(jnp.float32)
        swapped = jnp.concatenate([wide[:, half:], wide[:, :half]], axis=1)
        return (wide * cos_ref[rows, :] + swapped * sin_ref[rows, :]).astype(jnp.bfloat16)

    spans = ((low_ref, 0, HALF_WIN), (kv_ref, HALF_WIN, 512), (high_ref, 512 + HALF_WIN, HALF_WIN))
    for ref, at, count in spans:
        rows = pl.ds(at, count)
        k_scr[rows, :] = turn(ref[0], rows)
        value = ref[1].astype(jnp.float32)
        vt_scr[:, rows] = jnp.concatenate([value, value], axis=1).T.astype(jnp.bfloat16)
    start = (lax.axis_index("z") * 2 + lax.axis_index("co")) * 512
    key_at = lax.broadcasted_iota(jnp.int32, (384, 128), 0) - HALF_WIN
    gap = key_at - lax.broadcasted_iota(jnp.int32, (384, 128), 1)
    sink = sink_ref[0]
    for j in range(4):
        query = turn(q_ref[pl.ds(j * 128, 128), :], pl.ds(HALF_WIN + j * 128, 128))
        scores = lax.dot_general(
            k_scr[pl.ds(j * 128, 384), :], query, (((1,), (1,)), ((), ())),
            preferred_element_type=jnp.float32,
        ) * HEAD_DIM ** (-0.5)
        key = key_at + (start + j * 128)
        allowed = (jnp.abs(gap) <= HALF_WIN) & (key >= 0) & (key < 16384)
        scores = jnp.where(allowed, scores, NEG_BIG)
        peak = jnp.maximum(jnp.max(scores, axis=0, keepdims=True), sink)
        lifted = jnp.exp(scores - peak)
        total = jnp.sum(lifted, axis=0, keepdims=True) + jnp.exp(sink - peak)
        probs = (lifted / total).astype(jnp.bfloat16)
        mixed = jnp.dot(
            vt_scr[pl.ds(0, HEAD_DIM), pl.ds(j * 128, 384)], probs,
            preferred_element_type=jnp.float32,
        )
        out_ref[:, pl.ds(j * 128, 128)] = mixed.astype(jnp.bfloat16)


def attend(query_proj, key_proj, value_proj, sink_logit):
    kv_at = lax.axis_index("y") * HEAD_DIM
    own = jnp.stack(
        [lax.dynamic_slice_in_dim(a, kv_at, HEAD_DIM, 1) for a in (key_proj, value_proj)]
    )
    count = lax.axis_size(EP)
    forward = [(i, i + 1) for i in range(count - 1)]
    backward = [(target, source) for source, target in forward]
    low = lax.ppermute(own[:, 512 - HALF_WIN :], EP, forward)
    high = lax.ppermute(own[:, :HALF_WIN], EP, backward)
    offset = lax.axis_index(EP) * 512 - HALF_WIN
    half = HEAD_DIM // 2
    channel = jnp.arange(HEAD_DIM, dtype=jnp.int32)
    inverse_freq = 1.0 / ROPE_BASE ** ((channel % half).astype(jnp.float32) * 2.0 / HEAD_DIM)
    position = (jnp.arange(512 + 2 * HALF_WIN, dtype=jnp.int32) + offset).astype(jnp.float32)
    angles = position[:, None] * inverse_freq[None, :]
    cosine = jnp.cos(angles)
    sine = jnp.where(channel < half, -1.0, 1.0)[None, :] * jnp.sin(angles)
    return pl.pallas_call(
        attend_kernel,
        out_shape=jax.ShapeDtypeStruct((HEAD_DIM, 512), jnp.bfloat16),
        in_specs=[VMEM] * 6 + [pl.BlockSpec(memory_space=pltpu.SMEM)],
        out_specs=VMEM,
        scratch_shapes=[
            pltpu.VMEM((768, HEAD_DIM), jnp.bfloat16), pltpu.VMEM((128, 768), jnp.bfloat16)
        ],
        compiler_params=vmem_mib(12),
        name="attend",
    )(*(resident(a) for a in (query_proj, own, low, high, cosine, sine)), sink_logit)


def local(
    query_proj,
    key_proj,
    value_proj,
    sink_logit,
    out_weight,
    expert_input,
    norm_gain,
    routes,
    route_weights,
    gate_weight,
    up_weight,
    down_weight,
):
    wa = pack(PIECES_A, gate_weight, up_weight)
    prev_a = line_shift(wa, 1)
    next_a = line_shift(wa, -1)
    wb = pack(PIECES_B, up_weight, down_weight)
    next_b = line_shift(wb, -1)
    prev_b = line_shift(wb, 1)
    outgoing, slots = prepare(expert_input, norm_gain, routes)
    arrived = lax.all_to_all(outgoing, EP, 0, 0, tiled=True)
    far_a = line_shift(prev_a, 1)
    far_b = line_shift(next_b, -1)

    attended = attend(query_proj, key_proj, value_proj, sink_logit)

    payload = jnp.concatenate([arrived, attended], axis=0)
    rows = lax.all_to_all(
        jnp.broadcast_to(payload[None], (4, *payload.shape)),
        PLANE, 0, 0, tiled=True, axis_index_groups=LINE_M,
    )
    partial = ffn(rows, (wa, wb, prev_a, prev_b, next_a, next_b, far_a, far_b))
    parts = lax.all_to_all(partial, PLANE, 0, 0, tiled=True, axis_index_groups=WHOLE)
    result = total(parts).reshape(EXPERTS, CAP, 128)
    returned = lax.all_to_all(result, EP, 0, 0, tiled=True)
    expert_out = combine(returned.reshape(EXPERTS * CAP, 128), slots, route_weights)

    heads = rows[:, 256:]
    around = [line_shift(heads, step) for step in (1, -1, 2)]
    mixer_out = project(heads, *around, out_weight)
    return (mixer_out, expert_out)


def solution(mesh):
    finer = Mesh(mesh.devices.reshape(16, 2, 4, 4), ("z", "co", "y", "x"))
    in_specs = (
        P(EP, TP),
        P(EP, None),
        P(EP, None),
        P(TP),
        P(None, TP),
        P(EP, None),
        P(),
        P(EP, None),
        P(EP, None),
        P(EP, None, TP),
        P(EP, None, TP),
        P(EP, TP, None),
    )
    out_specs = (P(EP, TP), P(EP, TP))
    return jax.shard_map(local, mesh=finer, in_specs=in_specs, out_specs=out_specs, check_vma=False)
```

```python
import jax
import jax.numpy as jnp
from jax import lax
from jax.experimental import pallas as pl
from jax.experimental.pallas import tpu as pltpu
from jax.sharding import Mesh
from jax.sharding import PartitionSpec as P


D = 2048
HEAD_DIM = 64
HALF_WIN = 128
ROWS_B = 256
EXPERTS = 32
CAP = 32
EP = ("z", "co")
TP = ("y", "x")
PLANE = ("co", "y", "x")

NORM_EPS = 1e-06
ROPE_BASE = 10000.0
NEG_BIG = -1e30

LINE_L = [[y * 4 + x for x in range(4)] for y in range(4)] + [
    [16 + y * 4 + x for y in range(4)] for x in range(4)
]
LINE_M = [[y * 4 + x for y in range(4)] for x in range(4)] + [
    [16 + y * 4 + x for x in range(4)] for y in range(4)
]
WHOLE = [list(range(16)), [16 + (p % 4) * 4 + p // 4 for p in range(16)]]


ANY = pl.BlockSpec(memory_space=pl.ANY)
VMEM = pl.BlockSpec(memory_space=pltpu.VMEM)
IN_HBM = pl.BlockSpec(memory_space=pltpu.HBM)
HALF_W = 3072


def resident(x):
    return pltpu.with_memory_space_constraint(x, pltpu.VMEM)


def in_hbm(x):
    return pltpu.with_memory_space_constraint(x, pltpu.HBM)


def vmem_mib(count):
    return pltpu.CompilerParams(vmem_limit_bytes=count << 20)


def line_shift(x, step):
    pairs = [(line[i], line[(i + step) % 4]) for line in LINE_L for i in range(4)]
    return lax.ppermute(x, PLANE, pairs)


def pack_kernel(gate_ref, up_ref, down_ref, wa_ref, wb_ref, sems):
    copies = [
        (gate_ref.at[0], wa_ref.at[pl.ds(0, 2048)]),
        (up_ref.at[0, pl.ds(0, 1024)], wa_ref.at[pl.ds(2048, 1024)]),
        (up_ref.at[0, pl.ds(1024, 1024)], wb_ref.at[pl.ds(0, 1024)]),
    ] + [
        (down_ref.at[0, :, pl.ds(c * 256, 256)], wb_ref.at[pl.ds(1024 + c * 256, 256)])
        for c in range(8)
    ]
    copies = [pltpu.make_async_copy(s, d, sems.at[i]) for i, (s, d) in enumerate(copies)]
    for copy in copies:
        copy.start()
    for copy in copies:
        copy.wait()


def pack(gate, up, down):
    half = pltpu.VMEM((HALF_W, 256), jnp.bfloat16)
    return pl.pallas_call(
        pack_kernel,
        out_shape=(half, half),
        in_specs=[IN_HBM] * 3,
        out_specs=(VMEM, VMEM),
        scratch_shapes=[pltpu.SemaphoreType.DMA((11,))],
        compiler_params=vmem_mib(8),
        name="pack",
    )(*(in_hbm(a) for a in (gate, up, down)))


def prep_kernel(x_ref, gain_ref, routes_ref, out_ref, slot_ref, normed_ref):
    def norm_rows(i, carry):
        rows = pl.ds(pl.multiple_of(i * 32, 32), 32)
        wide = x_ref[rows, :].astype(jnp.float32)
        scale = lax.rsqrt(jnp.mean(wide * wide, axis=1, keepdims=True) + NORM_EPS)
        normed_ref[rows, :] = (wide * scale * gain_ref[...]).astype(jnp.bfloat16)
        return carry

    lax.fori_loop(0, ROWS_B // 32, norm_rows, 0)

    first = routes_ref[0:1, :]
    second = routes_ref[1:2, :]
    expert = lax.broadcasted_iota(jnp.int32, (128, ROWS_B), 0)
    row = lax.broadcasted_iota(jnp.int32, (ROWS_B, ROWS_B), 0)
    col = lax.broadcasted_iota(jnp.int32, (ROWS_B, ROWS_B), 1)
    above = jnp.where(row < col, 1.0, 0.0).astype(jnp.bfloat16)
    named = jnp.where((first == expert) | (second == expert), 1.0, 0.0)
    rank = jnp.dot(named.astype(jnp.bfloat16), above, preferred_element_type=jnp.float32)
    rank_a = jnp.sum(jnp.where(first == expert, rank, 0.0), axis=0, keepdims=True)
    rank_b = jnp.sum(jnp.where(second == expert, rank, 0.0), axis=0, keepdims=True)
    slot_a = first * CAP + rank_a.astype(jnp.int32)
    slot_b = second * CAP + rank_b.astype(jnp.int32)
    both = jnp.where(expert == 0, slot_a, slot_b).astype(jnp.float32)
    slot_ref[...] = both.T.astype(jnp.int32)

    mark = jnp.where(named > 0.5, rank, -1.0).astype(jnp.bfloat16)
    spread = jnp.where(
        (lax.broadcasted_iota(jnp.int32, (ROWS_B, 128), 0) >> 3)
        == lax.broadcasted_iota(jnp.int32, (ROWS_B, 128), 1),
        1.0,
        0.0,
    ).astype(jnp.bfloat16)
    mark_rows = jnp.dot(spread, mark, preferred_element_type=jnp.float32)
    xi = lax.axis_index("x")
    yi = lax.axis_index("y")
    even = ((row >> 3) & 1) == 0
    wanted = jnp.where(even, xi, yi) * 8 + (row & 7)
    pick = jnp.where(mark_rows.astype(jnp.int32) == wanted, 1.0, 0.0).astype(jnp.bfloat16)
    from_y = jnp.dot(
        pick, normed_ref[:, pl.ds(pl.multiple_of(yi * 512, 512), 512)],
        preferred_element_type=jnp.float32,
    )
    from_x = jnp.dot(
        pick, normed_ref[:, pl.ds(pl.multiple_of(xi * 512, 512), 512)],
        preferred_element_type=jnp.float32,
    )
    even_row = ((lax.broadcasted_iota(jnp.int32, (ROWS_B, 512), 0) >> 3) & 1) == 0
    out_ref[...] = jnp.where(even_row, from_y, from_x).astype(jnp.bfloat16)


def prepare(expert_input, norm_gain, routes):
    return pl.pallas_call(
        prep_kernel,
        out_shape=(
            jax.ShapeDtypeStruct((ROWS_B, 512), jnp.bfloat16),
            jax.ShapeDtypeStruct((ROWS_B, 128), jnp.int32),
        ),
        in_specs=[VMEM] * 3,
        out_specs=(VMEM, VMEM),
        scratch_shapes=[pltpu.VMEM((ROWS_B, D), jnp.bfloat16)],
        compiler_params=vmem_mib(16),
        name="prep",
    )(expert_input, norm_gain.reshape(1, D), routes.T)


def slice_hidden(x_ref, wa, wb):
    def part(m, ref, start):
        return jnp.dot(
            x_ref[m, pl.ds(0, ROWS_B), :], ref[pl.ds(start, 512), :],
            preferred_element_type=jnp.float32,
        )

    gate = part(0, wa, 0) + part(1, wa, 512) + part(2, wa, 1024) + part(3, wa, 1536)
    up = part(0, wa, 2048) + part(1, wa, 2560) + part(2, wb, 0) + part(3, wb, 512)
    return (gate / (1.0 + jnp.exp(-gate)) * up).astype(jnp.bfloat16)


def ffn_kernel(x_ref, *refs):
    weights, out_ref, acc_ref, bufs, sems, piece_ref, out_sems = refs[:8], *refs[8:]
    copies = [pltpu.make_async_copy(w, bufs.at[i], sems.at[i]) for i, w in enumerate(weights)]
    for copy in copies:
        copy.start()
    core = lax.axis_index("co")
    leave = []
    for s in range(4):
        copies[2 * s].wait()
        copies[2 * s + 1].wait()
        wa, wb = bufs.at[2 * s], bufs.at[2 * s + 1]
        hidden = slice_hidden(x_ref, wa, wb)
        for c in range(8):
            cols = pl.ds(c * 256, 256)
            term = jnp.dot(
                hidden, wb[pl.ds(1024 + c * 256, 256), :], preferred_element_type=jnp.float32
            )
            total = term if s == 0 else acc_ref[:, cols] + term
            if s < 3:
                acc_ref[:, cols] = total
                continue
            for k in range(2):
                t = 2 * c + k
                place = jnp.where(core == 0, t, (t % 4) * 4 + t // 4)
                piece_ref[t] = total[:, k * 128 : (k + 1) * 128].astype(jnp.bfloat16)
                leave.append(
                    pltpu.make_async_copy(piece_ref.at[t], out_ref.at[place], out_sems.at[t])
                )
                leave[-1].start()
    for copy in leave:
        copy.wait()


def ffn(x, weights):
    return pl.pallas_call(
        ffn_kernel,
        out_shape=pltpu.HBM((16, ROWS_B, 128), jnp.bfloat16),
        in_specs=[VMEM] + [ANY] * 8,
        out_specs=IN_HBM,
        scratch_shapes=[
            pltpu.VMEM((ROWS_B, D), jnp.float32),
            pltpu.VMEM((8, HALF_W, 256), jnp.bfloat16),
            pltpu.SemaphoreType.DMA((8,)),
            pltpu.VMEM((16, ROWS_B, 128), jnp.bfloat16),
            pltpu.SemaphoreType.DMA((16,)),
        ],
        compiler_params=vmem_mib(24),
        name="ffn",
    )(resident(x), *weights)


def total_kernel(parts_ref, out_ref):
    for l in range(4):
        rows = sum(parts_ref[4 * m + l].astype(jnp.float32) for m in range(4))
        out_ref[:, l] = rows.astype(jnp.bfloat16).reshape(EXPERTS, 8, 128)


def total(parts):
    return pl.pallas_call(
        total_kernel,
        out_shape=pltpu.VMEM((EXPERTS, 4, 8, 128), jnp.bfloat16),
        in_specs=[VMEM],
        out_specs=VMEM,
        compiler_params=vmem_mib(8),
        name="total",
    )(resident(parts))


def combine_kernel(ret_ref, slot_ref, weight_ref, out_ref):
    place = lax.broadcasted_iota(jnp.int32, (ROWS_B, EXPERTS * CAP), 1)
    total = None
    for k in range(2):
        pick = jnp.where(place == slot_ref[:, k : k + 1], 1.0, 0.0).astype(jnp.bfloat16)
        rows = jnp.dot(pick, ret_ref[...], preferred_element_type=jnp.float32)
        term = rows * weight_ref[:, k : k + 1]
        total = term if total is None else total + term
    out_ref[...] = total.astype(jnp.bfloat16)


def combine(returned, slots, route_weights):
    return pl.pallas_call(
        combine_kernel,
        out_shape=jax.ShapeDtypeStruct((ROWS_B, 128), jnp.bfloat16),
        in_specs=[VMEM] * 3,
        out_specs=VMEM,
        compiler_params=vmem_mib(12),
        name="combine",
    )(resident(returned), slots, route_weights)


def project_kernel(own_ref, prev_ref, next_ref, far_ref, weight_ref, out_ref, a_ref):
    core = lax.axis_index("co")
    line = jnp.where(core == 0, lax.axis_index("x"), lax.axis_index("y"))
    for ref, step in ((own_ref, 0), (prev_ref, 3), (next_ref, 1), (far_ref, 2)):
        source = lax.rem(line + step, 4)
        for m in range(4):
            head = jnp.where(core == 0, m * 4 + source, source * 4 + m)
            a_ref[pl.ds(pl.multiple_of(head * HEAD_DIM, HEAD_DIM), HEAD_DIM), :] = ref[m]
    turned = weight_ref[...].astype(jnp.float32).T.astype(jnp.bfloat16)
    out = jnp.dot(turned, a_ref[...], preferred_element_type=jnp.float32)
    out_ref[...] = out.T.astype(jnp.bfloat16)


def project(own, prev, nxt, far, out_weight):
    return pl.pallas_call(
        project_kernel,
        out_shape=jax.ShapeDtypeStruct((512, 128), jnp.bfloat16),
        in_specs=[VMEM] * 5,
        out_specs=VMEM,
        scratch_shapes=[pltpu.VMEM((1024, 512), jnp.bfloat16)],
        compiler_params=vmem_mib(12),
        name="project",
    )(*(resident(a) for a in (own, prev, nxt, far, out_weight)))


def attend_kernel(q_ref, kv_ref, low_ref, high_ref, cos_ref, sin_ref, sink_ref, out_ref,
                  k_scr, vt_scr):
    half = HEAD_DIM // 2

    def turn(x, rows):
        wide = x.astype(jnp.float32)
        swapped = jnp.concatenate([wide[:, half:], wide[:, :half]], axis=1)
        return (wide * cos_ref[rows, :] + swapped * sin_ref[rows, :]).astype(jnp.bfloat16)

    spans = ((low_ref, 0, HALF_WIN), (kv_ref, HALF_WIN, 512), (high_ref, 512 + HALF_WIN, HALF_WIN))
    for ref, at, count in spans:
        rows = pl.ds(at, count)
        k_scr[rows, :] = turn(ref[0], rows)
        value = ref[1].astype(jnp.float32)
        vt_scr[:, rows] = jnp.concatenate([value, value], axis=1).T.astype(jnp.bfloat16)
    start = (lax.axis_index("z") * 2 + lax.axis_index("co")) * 512
    key_at = lax.broadcasted_iota(jnp.int32, (384, 128), 0) - HALF_WIN
    gap = key_at - lax.broadcasted_iota(jnp.int32, (384, 128), 1)
    sink = sink_ref[0]
    for j in range(4):
        query = turn(q_ref[pl.ds(j * 128, 128), :], pl.ds(HALF_WIN + j * 128, 128))
        scores = lax.dot_general(
            k_scr[pl.ds(j * 128, 384), :], query, (((1,), (1,)), ((), ())),
            preferred_element_type=jnp.float32,
        ) * HEAD_DIM ** (-0.5)
        key = key_at + (start + j * 128)
        allowed = (jnp.abs(gap) <= HALF_WIN) & (key >= 0) & (key < 16384)
        scores = jnp.where(allowed, scores, NEG_BIG)
        peak = jnp.maximum(jnp.max(scores, axis=0, keepdims=True), sink)
        lifted = jnp.exp(scores - peak)
        total = jnp.sum(lifted, axis=0, keepdims=True) + jnp.exp(sink - peak)
        probs = (lifted / total).astype(jnp.bfloat16)
        mixed = jnp.dot(
            vt_scr[pl.ds(0, HEAD_DIM), pl.ds(j * 128, 384)], probs,
            preferred_element_type=jnp.float32,
        )
        out_ref[:, pl.ds(j * 128, 128)] = mixed.astype(jnp.bfloat16)


def attend(query_proj, key_proj, value_proj, sink_logit):
    kv_at = lax.axis_index("y") * HEAD_DIM
    own = jnp.stack(
        [lax.dynamic_slice_in_dim(a, kv_at, HEAD_DIM, 1) for a in (key_proj, value_proj)]
    )
    count = lax.axis_size(EP)
    forward = [(i, i + 1) for i in range(count - 1)]
    backward = [(target, source) for source, target in forward]
    low = lax.ppermute(own[:, 512 - HALF_WIN :], EP, forward)
    high = lax.ppermute(own[:, :HALF_WIN], EP, backward)
    offset = lax.axis_index(EP) * 512 - HALF_WIN
    half = HEAD_DIM // 2
    channel = jnp.arange(HEAD_DIM, dtype=jnp.int32)
    inverse_freq = 1.0 / ROPE_BASE ** ((channel % half).astype(jnp.float32) * 2.0 / HEAD_DIM)
    position = (jnp.arange(512 + 2 * HALF_WIN, dtype=jnp.int32) + offset).astype(jnp.float32)
    angles = position[:, None] * inverse_freq[None, :]
    cosine = jnp.cos(angles)
    sine = jnp.where(channel < half, -1.0, 1.0)[None, :] * jnp.sin(angles)
    return pl.pallas_call(
        attend_kernel,
        out_shape=jax.ShapeDtypeStruct((HEAD_DIM, 512), jnp.bfloat16),
        in_specs=[VMEM] * 6 + [pl.BlockSpec(memory_space=pltpu.SMEM)],
        out_specs=VMEM,
        scratch_shapes=[
            pltpu.VMEM((768, HEAD_DIM), jnp.bfloat16), pltpu.VMEM((128, 768), jnp.bfloat16)
        ],
        compiler_params=vmem_mib(12),
        name="attend",
    )(*(resident(a) for a in (query_proj, own, low, high, cosine, sine)), sink_logit)


def local(
    query_proj,
    key_proj,
    value_proj,
    sink_logit,
    out_weight,
    expert_input,
    norm_gain,
    routes,
    route_weights,
    gate_weight,
    up_weight,
    down_weight,
):
    wa, wb = pack(gate_weight, up_weight, down_weight)
    prev_a = line_shift(wa, 1)
    next_b = line_shift(wb, -1)
    next_a = line_shift(wa, -1)
    prev_b = line_shift(wb, 1)
    outgoing, slots = prepare(expert_input, norm_gain, routes)
    arrived = lax.all_to_all(outgoing, EP, 0, 0, tiled=True)
    far_a = line_shift(prev_a, 1)
    far_b = line_shift(next_b, -1)

    attended = attend(query_proj, key_proj, value_proj, sink_logit)

    payload = jnp.concatenate([arrived, attended], axis=0)
    rows = lax.all_to_all(
        jnp.broadcast_to(payload[None], (4, *payload.shape)),
        PLANE, 0, 0, tiled=True, axis_index_groups=LINE_M,
    )
    partial = ffn(rows, (wa, wb, prev_a, prev_b, next_a, next_b, far_a, far_b))
    parts = lax.all_to_all(partial, PLANE, 0, 0, tiled=True, axis_index_groups=WHOLE)
    result = total(parts).reshape(EXPERTS, CAP, 128)
    returned = lax.all_to_all(result, EP, 0, 0, tiled=True)
    expert_out = combine(returned.reshape(EXPERTS * CAP, 128), slots, route_weights)

    heads = rows[:, 256:]
    near = [line_shift(heads, step) for step in (1, -1)]
    far = line_shift(heads, 2)
    mixer_out = project(heads, *near, far, out_weight)
    return (mixer_out, expert_out)


def solution(mesh):
    finer = Mesh(mesh.devices.reshape(16, 2, 4, 4), ("z", "co", "y", "x"))
    in_specs = (
        P(EP, TP),
        P(EP, None),
        P(EP, None),
        P(TP),
        P(None, TP),
        P(EP, None),
        P(),
        P(EP, None),
        P(EP, None),
        P(EP, None, TP),
        P(EP, None, TP),
        P(EP, TP, None),
    )
    out_specs = (P(EP, TP), P(EP, TP))
    return jax.shard_map(local, mesh=finer, in_specs=in_specs, out_specs=out_specs, check_vma=False)
```

```python
import jax
import jax.numpy as jnp
from jax import lax
from jax.experimental import pallas as pl
from jax.experimental.pallas import tpu as pltpu
from jax.sharding import Mesh
from jax.sharding import PartitionSpec as P


D = 2048
HEAD_DIM = 64
HALF_WIN = 128
ROWS_B = 256
EXPERTS = 32
CAP = 32
EP = ("z", "co")
TP = ("y", "x")
PLANE = ("co", "y", "x")

NORM_EPS = 1e-06
ROPE_BASE = 10000.0
NEG_BIG = -1e30

LINE_L = [[y * 4 + x for x in range(4)] for y in range(4)] + [
    [16 + y * 4 + x for y in range(4)] for x in range(4)
]
LINE_M = [[y * 4 + x for y in range(4)] for x in range(4)] + [
    [16 + y * 4 + x for x in range(4)] for y in range(4)
]
WHOLE = [list(range(16)), [16 + (p % 4) * 4 + p // 4 for p in range(16)]]


ANY = pl.BlockSpec(memory_space=pl.ANY)
VMEM = pl.BlockSpec(memory_space=pltpu.VMEM)
IN_HBM = pl.BlockSpec(memory_space=pltpu.HBM)
HALF_W = 3072


def resident(x):
    return pltpu.with_memory_space_constraint(x, pltpu.VMEM)


def in_hbm(x):
    return pltpu.with_memory_space_constraint(x, pltpu.HBM)


def vmem_mib(count):
    return pltpu.CompilerParams(vmem_limit_bytes=count << 20)


NEAR_A = (1, 0, 3, 2)
NEAR_B = (3, 2, 1, 0)
ACROSS = (2, 3, 0, 1)


def swap(x, partner):
    pairs = [(line[i], line[partner[i]]) for line in LINE_L for i in range(4)]
    return lax.ppermute(x, PLANE, pairs)


def pack_kernel(gate_ref, up_ref, down_ref, wa_ref, wb_ref, sems):
    copies = [
        (gate_ref.at[0], wa_ref.at[pl.ds(0, 2048)]),
        (up_ref.at[0, pl.ds(0, 1024)], wa_ref.at[pl.ds(2048, 1024)]),
        (up_ref.at[0, pl.ds(1024, 1024)], wb_ref.at[pl.ds(0, 1024)]),
    ] + [
        (down_ref.at[0, :, pl.ds(c * 256, 256)], wb_ref.at[pl.ds(1024 + c * 256, 256)])
        for c in range(8)
    ]
    copies = [pltpu.make_async_copy(s, d, sems.at[i]) for i, (s, d) in enumerate(copies)]
    for copy in copies:
        copy.start()
    for copy in copies:
        copy.wait()


def pack(gate, up, down):
    half = pltpu.VMEM((HALF_W, 256), jnp.bfloat16)
    return pl.pallas_call(
        pack_kernel,
        out_shape=(half, half),
        in_specs=[IN_HBM] * 3,
        out_specs=(VMEM, VMEM),
        scratch_shapes=[pltpu.SemaphoreType.DMA((11,))],
        compiler_params=vmem_mib(8),
        name="pack",
    )(*(in_hbm(a) for a in (gate, up, down)))


def prep_kernel(x_ref, gain_ref, routes_ref, out_ref, slot_ref, normed_ref):
    def norm_rows(i, carry):
        rows = pl.ds(pl.multiple_of(i * 32, 32), 32)
        wide = x_ref[rows, :].astype(jnp.float32)
        scale = lax.rsqrt(jnp.mean(wide * wide, axis=1, keepdims=True) + NORM_EPS)
        normed_ref[rows, :] = (wide * scale * gain_ref[...]).astype(jnp.bfloat16)
        return carry

    lax.fori_loop(0, ROWS_B // 32, norm_rows, 0)

    first = routes_ref[0:1, :]
    second = routes_ref[1:2, :]
    expert = lax.broadcasted_iota(jnp.int32, (128, ROWS_B), 0)
    row = lax.broadcasted_iota(jnp.int32, (ROWS_B, ROWS_B), 0)
    col = lax.broadcasted_iota(jnp.int32, (ROWS_B, ROWS_B), 1)
    above = jnp.where(row < col, 1.0, 0.0).astype(jnp.bfloat16)
    named = jnp.where((first == expert) | (second == expert), 1.0, 0.0)
    rank = jnp.dot(named.astype(jnp.bfloat16), above, preferred_element_type=jnp.float32)
    rank_a = jnp.sum(jnp.where(first == expert, rank, 0.0), axis=0, keepdims=True)
    rank_b = jnp.sum(jnp.where(second == expert, rank, 0.0), axis=0, keepdims=True)
    slot_a = first * CAP + rank_a.astype(jnp.int32)
    slot_b = second * CAP + rank_b.astype(jnp.int32)
    both = jnp.where(expert == 0, slot_a, slot_b).astype(jnp.float32)
    slot_ref[...] = both.T.astype(jnp.int32)

    mark = jnp.where(named > 0.5, rank, -1.0).astype(jnp.bfloat16)
    spread = jnp.where(
        (lax.broadcasted_iota(jnp.int32, (ROWS_B, 128), 0) >> 3)
        == lax.broadcasted_iota(jnp.int32, (ROWS_B, 128), 1),
        1.0,
        0.0,
    ).astype(jnp.bfloat16)
    mark_rows = jnp.dot(spread, mark, preferred_element_type=jnp.float32)
    xi = lax.axis_index("x")
    yi = lax.axis_index("y")
    even = ((row >> 3) & 1) == 0
    wanted = jnp.where(even, xi, yi) * 8 + (row & 7)
    pick = jnp.where(mark_rows.astype(jnp.int32) == wanted, 1.0, 0.0).astype(jnp.bfloat16)
    from_y = jnp.dot(
        pick, normed_ref[:, pl.ds(pl.multiple_of(yi * 512, 512), 512)],
        preferred_element_type=jnp.float32,
    )
    from_x = jnp.dot(
        pick, normed_ref[:, pl.ds(pl.multiple_of(xi * 512, 512), 512)],
        preferred_element_type=jnp.float32,
    )
    even_row = ((lax.broadcasted_iota(jnp.int32, (ROWS_B, 512), 0) >> 3) & 1) == 0
    out_ref[...] = jnp.where(even_row, from_y, from_x).astype(jnp.bfloat16)


def prepare(expert_input, norm_gain, routes):
    return pl.pallas_call(
        prep_kernel,
        out_shape=(
            jax.ShapeDtypeStruct((ROWS_B, 512), jnp.bfloat16),
            jax.ShapeDtypeStruct((ROWS_B, 128), jnp.int32),
        ),
        in_specs=[VMEM] * 3,
        out_specs=(VMEM, VMEM),
        scratch_shapes=[pltpu.VMEM((ROWS_B, D), jnp.bfloat16)],
        compiler_params=vmem_mib(16),
        name="prep",
    )(expert_input, norm_gain.reshape(1, D), routes.T)


def slice_hidden(x_ref, wa, wb):
    def part(m, ref, start):
        return jnp.dot(
            x_ref[m, pl.ds(0, ROWS_B), :], ref[pl.ds(start, 512), :],
            preferred_element_type=jnp.float32,
        )

    gate = part(0, wa, 0) + part(1, wa, 512) + part(2, wa, 1024) + part(3, wa, 1536)
    up = part(0, wa, 2048) + part(1, wa, 2560) + part(2, wb, 0) + part(3, wb, 512)
    return (gate / (1.0 + jnp.exp(-gate)) * up).astype(jnp.bfloat16)


def ffn_kernel(x_ref, *refs):
    weights, out_ref, acc_ref, bufs, sems, piece_ref, out_sems = refs[:8], *refs[8:]
    copies = [pltpu.make_async_copy(w, bufs.at[i], sems.at[i]) for i, w in enumerate(weights)]
    for copy in copies:
        copy.start()
    core = lax.axis_index("co")
    leave = []
    for s in range(4):
        copies[2 * s].wait()
        copies[2 * s + 1].wait()
        wa, wb = bufs.at[2 * s], bufs.at[2 * s + 1]
        hidden = slice_hidden(x_ref, wa, wb)
        for c in range(8):
            cols = pl.ds(c * 256, 256)
            term = jnp.dot(
                hidden, wb[pl.ds(1024 + c * 256, 256), :], preferred_element_type=jnp.float32
            )
            total = term if s == 0 else acc_ref[:, cols] + term
            if s < 3:
                acc_ref[:, cols] = total
                continue
            for k in range(2):
                t = 2 * c + k
                place = jnp.where(core == 0, t, (t % 4) * 4 + t // 4)
                piece_ref[t] = total[:, k * 128 : (k + 1) * 128].astype(jnp.bfloat16)
                leave.append(
                    pltpu.make_async_copy(piece_ref.at[t], out_ref.at[place], out_sems.at[t])
                )
                leave[-1].start()
    for copy in leave:
        copy.wait()


def ffn(x, weights):
    return pl.pallas_call(
        ffn_kernel,
        out_shape=pltpu.HBM((16, ROWS_B, 128), jnp.bfloat16),
        in_specs=[VMEM] + [ANY] * 8,
        out_specs=IN_HBM,
        scratch_shapes=[
            pltpu.VMEM((ROWS_B, D), jnp.float32),
            pltpu.VMEM((8, HALF_W, 256), jnp.bfloat16),
            pltpu.SemaphoreType.DMA((8,)),
            pltpu.VMEM((16, ROWS_B, 128), jnp.bfloat16),
            pltpu.SemaphoreType.DMA((16,)),
        ],
        compiler_params=vmem_mib(24),
        name="ffn",
    )(resident(x), *weights)


def total_kernel(parts_ref, out_ref):
    for l in range(4):
        rows = sum(parts_ref[4 * m + l].astype(jnp.float32) for m in range(4))
        out_ref[:, l] = rows.astype(jnp.bfloat16).reshape(EXPERTS, 8, 128)


def total(parts):
    return pl.pallas_call(
        total_kernel,
        out_shape=pltpu.VMEM((EXPERTS, 4, 8, 128), jnp.bfloat16),
        in_specs=[VMEM],
        out_specs=VMEM,
        compiler_params=vmem_mib(8),
        name="total",
    )(resident(parts))


def combine_kernel(ret_ref, slot_ref, weight_ref, out_ref):
    place = lax.broadcasted_iota(jnp.int32, (ROWS_B, EXPERTS * CAP), 1)
    total = None
    for k in range(2):
        pick = jnp.where(place == slot_ref[:, k : k + 1], 1.0, 0.0).astype(jnp.bfloat16)
        rows = jnp.dot(pick, ret_ref[...], preferred_element_type=jnp.float32)
        term = rows * weight_ref[:, k : k + 1]
        total = term if total is None else total + term
    out_ref[...] = total.astype(jnp.bfloat16)


def combine(returned, slots, route_weights):
    return pl.pallas_call(
        combine_kernel,
        out_shape=jax.ShapeDtypeStruct((ROWS_B, 128), jnp.bfloat16),
        in_specs=[VMEM] * 3,
        out_specs=VMEM,
        compiler_params=vmem_mib(12),
        name="combine",
    )(resident(returned), slots, route_weights)


def project_kernel(own_ref, one_ref, two_ref, far_ref, weight_ref, out_ref, a_ref):
    core = lax.axis_index("co")
    line = jnp.where(core == 0, lax.axis_index("x"), lax.axis_index("y"))
    odd = lax.rem(line, 2)
    for ref, source in (
        (own_ref, line),
        (one_ref, line + 1 - 2 * odd),
        (two_ref, 3 - line),
        (far_ref, lax.rem(line + 2, 4)),
    ):
        for m in range(4):
            head = jnp.where(core == 0, m * 4 + source, source * 4 + m)
            a_ref[pl.ds(pl.multiple_of(head * HEAD_DIM, HEAD_DIM), HEAD_DIM), :] = ref[m]
    turned = weight_ref[...].astype(jnp.float32).T.astype(jnp.bfloat16)
    out = jnp.dot(turned, a_ref[...], preferred_element_type=jnp.float32)
    out_ref[...] = out.T.astype(jnp.bfloat16)


def project(own, one, two, far, out_weight):
    return pl.pallas_call(
        project_kernel,
        out_shape=jax.ShapeDtypeStruct((512, 128), jnp.bfloat16),
        in_specs=[VMEM] * 5,
        out_specs=VMEM,
        scratch_shapes=[pltpu.VMEM((1024, 512), jnp.bfloat16)],
        compiler_params=vmem_mib(12),
        name="project",
    )(*(resident(a) for a in (own, one, two, far, out_weight)))


def attend_kernel(q_ref, kv_ref, low_ref, high_ref, cos_ref, sin_ref, sink_ref, out_ref,
                  k_scr, vt_scr):
    half = HEAD_DIM // 2

    def turn(x, rows):
        wide = x.astype(jnp.float32)
        swapped = jnp.concatenate([wide[:, half:], wide[:, :half]], axis=1)
        return (wide * cos_ref[rows, :] + swapped * sin_ref[rows, :]).astype(jnp.bfloat16)

    spans = ((low_ref, 0, HALF_WIN), (kv_ref, HALF_WIN, 512), (high_ref, 512 + HALF_WIN, HALF_WIN))
    for ref, at, count in spans:
        rows = pl.ds(at, count)
        k_scr[rows, :] = turn(ref[0], rows)
        value = ref[1].astype(jnp.float32)
        vt_scr[:, rows] = jnp.concatenate([value, value], axis=1).T.astype(jnp.bfloat16)
    start = (lax.axis_index("z") * 2 + lax.axis_index("co")) * 512
    key_at = lax.broadcasted_iota(jnp.int32, (384, 128), 0) - HALF_WIN
    gap = key_at - lax.broadcasted_iota(jnp.int32, (384, 128), 1)
    sink = sink_ref[0]
    for j in range(4):
        query = turn(q_ref[pl.ds(j * 128, 128), :], pl.ds(HALF_WIN + j * 128, 128))
        scores = lax.dot_general(
            k_scr[pl.ds(j * 128, 384), :], query, (((1,), (1,)), ((), ())),
            preferred_element_type=jnp.float32,
        ) * HEAD_DIM ** (-0.5)
        key = key_at + (start + j * 128)
        allowed = (jnp.abs(gap) <= HALF_WIN) & (key >= 0) & (key < 16384)
        scores = jnp.where(allowed, scores, NEG_BIG)
        peak = jnp.maximum(jnp.max(scores, axis=0, keepdims=True), sink)
        lifted = jnp.exp(scores - peak)
        total = jnp.sum(lifted, axis=0, keepdims=True) + jnp.exp(sink - peak)
        probs = (lifted / total).astype(jnp.bfloat16)
        mixed = jnp.dot(
            vt_scr[pl.ds(0, HEAD_DIM), pl.ds(j * 128, 384)], probs,
            preferred_element_type=jnp.float32,
        )
        out_ref[:, pl.ds(j * 128, 128)] = mixed.astype(jnp.bfloat16)


def attend(query_proj, key_proj, value_proj, sink_logit):
    kv_at = lax.axis_index("y") * HEAD_DIM
    own = jnp.stack(
        [lax.dynamic_slice_in_dim(a, kv_at, HEAD_DIM, 1) for a in (key_proj, value_proj)]
    )
    count = lax.axis_size(EP)
    forward = [(i, i + 1) for i in range(count - 1)]
    backward = [(target, source) for source, target in forward]
    low = lax.ppermute(own[:, 512 - HALF_WIN :], EP, forward)
    high = lax.ppermute(own[:, :HALF_WIN], EP, backward)
    offset = lax.axis_index(EP) * 512 - HALF_WIN
    half = HEAD_DIM // 2
    channel = jnp.arange(HEAD_DIM, dtype=jnp.int32)
    inverse_freq = 1.0 / ROPE_BASE ** ((channel % half).astype(jnp.float32) * 2.0 / HEAD_DIM)
    position = (jnp.arange(512 + 2 * HALF_WIN, dtype=jnp.int32) + offset).astype(jnp.float32)
    angles = position[:, None] * inverse_freq[None, :]
    cosine = jnp.cos(angles)
    sine = jnp.where(channel < half, -1.0, 1.0)[None, :] * jnp.sin(angles)
    return pl.pallas_call(
        attend_kernel,
        out_shape=jax.ShapeDtypeStruct((HEAD_DIM, 512), jnp.bfloat16),
        in_specs=[VMEM] * 6 + [pl.BlockSpec(memory_space=pltpu.SMEM)],
        out_specs=VMEM,
        scratch_shapes=[
            pltpu.VMEM((768, HEAD_DIM), jnp.bfloat16), pltpu.VMEM((128, 768), jnp.bfloat16)
        ],
        compiler_params=vmem_mib(12),
        name="attend",
    )(*(resident(a) for a in (query_proj, own, low, high, cosine, sine)), sink_logit)


def local(
    query_proj,
    key_proj,
    value_proj,
    sink_logit,
    out_weight,
    expert_input,
    norm_gain,
    routes,
    route_weights,
    gate_weight,
    up_weight,
    down_weight,
):
    wa, wb = pack(gate_weight, up_weight, down_weight)
    one_a = swap(wa, NEAR_A)
    two_b = swap(wb, NEAR_B)
    one_b = swap(wb, NEAR_A)
    two_a = swap(wa, NEAR_B)
    outgoing, slots = prepare(expert_input, norm_gain, routes)
    arrived = lax.all_to_all(outgoing, EP, 0, 0, tiled=True)
    far_a = swap(one_a, NEAR_B)
    far_b = swap(two_b, NEAR_A)

    attended = attend(query_proj, key_proj, value_proj, sink_logit)

    payload = jnp.concatenate([arrived, attended], axis=0)
    rows = lax.all_to_all(
        jnp.broadcast_to(payload[None], (4, *payload.shape)),
        PLANE, 0, 0, tiled=True, axis_index_groups=LINE_M,
    )
    partial = ffn(rows, (wa, wb, one_a, one_b, two_a, two_b, far_a, far_b))
    parts = lax.all_to_all(partial, PLANE, 0, 0, tiled=True, axis_index_groups=WHOLE)
    result = total(parts).reshape(EXPERTS, CAP, 128)
    returned = lax.all_to_all(result, EP, 0, 0, tiled=True)
    expert_out = combine(returned.reshape(EXPERTS * CAP, 128), slots, route_weights)

    heads = rows[:, 256:]
    near = [swap(heads, partner) for partner in (NEAR_A, NEAR_B)]
    far = swap(heads, ACROSS)
    mixer_out = project(heads, *near, far, out_weight)
    return (mixer_out, expert_out)


def solution(mesh):
    finer = Mesh(mesh.devices.reshape(16, 2, 4, 4), ("z", "co", "y", "x"))
    in_specs = (
        P(EP, TP),
        P(EP, None),
        P(EP, None),
        P(TP),
        P(None, TP),
        P(EP, None),
        P(),
        P(EP, None),
        P(EP, None),
        P(EP, None, TP),
        P(EP, None, TP),
        P(EP, TP, None),
    )
    out_specs = (P(EP, TP), P(EP, TP))
    return jax.shard_map(local, mesh=finer, in_specs=in_specs, out_specs=out_specs, check_vma=False)
```

```python
import jax
import jax.numpy as jnp
from jax import lax
from jax.experimental import pallas as pl
from jax.experimental.pallas import tpu as pltpu
from jax.sharding import Mesh
from jax.sharding import PartitionSpec as P


D = 2048
HEAD_DIM = 64
HALF_WIN = 128
ROWS_B = 256
EXPERTS = 32
CAP = 32
EP = ("z", "co")
TP = ("y", "x")
PLANE = ("co", "y", "x")

NORM_EPS = 1e-06
ROPE_BASE = 10000.0
NEG_BIG = -1e30

LINE_L = [[y * 4 + x for x in range(4)] for y in range(4)] + [
    [16 + y * 4 + x for y in range(4)] for x in range(4)
]
LINE_M = [[y * 4 + x for y in range(4)] for x in range(4)] + [
    [16 + y * 4 + x for x in range(4)] for y in range(4)
]
WHOLE = [list(range(16)), [16 + (p % 4) * 4 + p // 4 for p in range(16)]]


ANY = pl.BlockSpec(memory_space=pl.ANY)
VMEM = pl.BlockSpec(memory_space=pltpu.VMEM)
IN_HBM = pl.BlockSpec(memory_space=pltpu.HBM)
HALF_W = 3072


def resident(x):
    return pltpu.with_memory_space_constraint(x, pltpu.VMEM)


def in_hbm(x):
    return pltpu.with_memory_space_constraint(x, pltpu.HBM)


def vmem_mib(count):
    return pltpu.CompilerParams(vmem_limit_bytes=count << 20)


NEAR_A = (1, 0, 3, 2)
NEAR_B = (3, 2, 1, 0)
ACROSS = (2, 3, 0, 1)


def swap(x, partner):
    pairs = [(line[i], line[partner[i]]) for line in LINE_L for i in range(4)]
    return lax.ppermute(x, PLANE, pairs)


def pack_kernel(gate_ref, up_ref, down_ref, wa_ref, wb_ref, stage_ref, sems, out_sems):
    second = [(up_ref.at[0, pl.ds(1024, 1024)], 0, 1024)] + [
        (down_ref.at[0, :, pl.ds(c * 256, 256)], 1024 + c * 256, 256) for c in range(8)
    ]
    come = [
        pltpu.make_async_copy(source, stage_ref.at[pl.ds(at, count)], sems.at[i])
        for i, (source, at, count) in enumerate(second)
    ]
    leave = [
        pltpu.make_async_copy(
            stage_ref.at[pl.ds(at, count)], wb_ref.at[pl.ds(at, count)], out_sems.at[i]
        )
        for i, (_, at, count) in enumerate(second)
    ]
    first = [
        pltpu.make_async_copy(gate_ref.at[0], wa_ref.at[pl.ds(0, 2048)], sems.at[9]),
        pltpu.make_async_copy(
            up_ref.at[0, pl.ds(0, 1024)], wa_ref.at[pl.ds(2048, 1024)], sems.at[10]
        ),
    ]
    for copy in come + first:
        copy.start()
    for arrival, departure in zip(come, leave):
        arrival.wait()
        departure.start()
    for copy in first + leave:
        copy.wait()


def pack(gate, up, down):
    return pl.pallas_call(
        pack_kernel,
        out_shape=(
            pltpu.VMEM((HALF_W, 256), jnp.bfloat16), pltpu.HBM((HALF_W, 256), jnp.bfloat16)
        ),
        in_specs=[IN_HBM] * 3,
        out_specs=(VMEM, IN_HBM),
        scratch_shapes=[
            pltpu.VMEM((HALF_W, 256), jnp.bfloat16),
            pltpu.SemaphoreType.DMA((11,)),
            pltpu.SemaphoreType.DMA((9,)),
        ],
        compiler_params=vmem_mib(8),
        name="pack",
    )(*(in_hbm(a) for a in (gate, up, down)))


def prep_kernel(x_ref, gain_ref, routes_ref, out_ref, slot_ref, normed_ref):
    def norm_rows(i, carry):
        rows = pl.ds(pl.multiple_of(i * 32, 32), 32)
        wide = x_ref[rows, :].astype(jnp.float32)
        scale = lax.rsqrt(jnp.mean(wide * wide, axis=1, keepdims=True) + NORM_EPS)
        normed_ref[rows, :] = (wide * scale * gain_ref[...]).astype(jnp.bfloat16)
        return carry

    lax.fori_loop(0, ROWS_B // 32, norm_rows, 0)

    first = routes_ref[0:1, :]
    second = routes_ref[1:2, :]
    expert = lax.broadcasted_iota(jnp.int32, (128, ROWS_B), 0)
    row = lax.broadcasted_iota(jnp.int32, (ROWS_B, ROWS_B), 0)
    col = lax.broadcasted_iota(jnp.int32, (ROWS_B, ROWS_B), 1)
    above = jnp.where(row < col, 1.0, 0.0).astype(jnp.bfloat16)
    named = jnp.where((first == expert) | (second == expert), 1.0, 0.0)
    rank = jnp.dot(named.astype(jnp.bfloat16), above, preferred_element_type=jnp.float32)
    rank_a = jnp.sum(jnp.where(first == expert, rank, 0.0), axis=0, keepdims=True)
    rank_b = jnp.sum(jnp.where(second == expert, rank, 0.0), axis=0, keepdims=True)
    slot_a = first * CAP + rank_a.astype(jnp.int32)
    slot_b = second * CAP + rank_b.astype(jnp.int32)
    both = jnp.where(expert == 0, slot_a, slot_b).astype(jnp.float32)
    slot_ref[...] = both.T.astype(jnp.int32)

    mark = jnp.where(named > 0.5, rank, -1.0).astype(jnp.bfloat16)
    spread = jnp.where(
        (lax.broadcasted_iota(jnp.int32, (ROWS_B, 128), 0) >> 3)
        == lax.broadcasted_iota(jnp.int32, (ROWS_B, 128), 1),
        1.0,
        0.0,
    ).astype(jnp.bfloat16)
    mark_rows = jnp.dot(spread, mark, preferred_element_type=jnp.float32)
    xi = lax.axis_index("x")
    yi = lax.axis_index("y")
    even = ((row >> 3) & 1) == 0
    wanted = jnp.where(even, xi, yi) * 8 + (row & 7)
    pick = jnp.where(mark_rows.astype(jnp.int32) == wanted, 1.0, 0.0).astype(jnp.bfloat16)
    from_y = jnp.dot(
        pick, normed_ref[:, pl.ds(pl.multiple_of(yi * 512, 512), 512)],
        preferred_element_type=jnp.float32,
    )
    from_x = jnp.dot(
        pick, normed_ref[:, pl.ds(pl.multiple_of(xi * 512, 512), 512)],
        preferred_element_type=jnp.float32,
    )
    even_row = ((lax.broadcasted_iota(jnp.int32, (ROWS_B, 512), 0) >> 3) & 1) == 0
    out_ref[...] = jnp.where(even_row, from_y, from_x).astype(jnp.bfloat16)


def prepare(expert_input, norm_gain, routes):
    return pl.pallas_call(
        prep_kernel,
        out_shape=(
            jax.ShapeDtypeStruct((ROWS_B, 512), jnp.bfloat16),
            jax.ShapeDtypeStruct((ROWS_B, 128), jnp.int32),
        ),
        in_specs=[VMEM] * 3,
        out_specs=(VMEM, VMEM),
        scratch_shapes=[pltpu.VMEM((ROWS_B, D), jnp.bfloat16)],
        compiler_params=vmem_mib(16),
        name="prep",
    )(expert_input, norm_gain.reshape(1, D), routes.T)


def slice_hidden(x_ref, wa, wb):
    def part(m, ref, start):
        return jnp.dot(
            x_ref[m, pl.ds(0, ROWS_B), :], ref[pl.ds(start, 512), :],
            preferred_element_type=jnp.float32,
        )

    gate = part(0, wa, 0) + part(1, wa, 512) + part(2, wa, 1024) + part(3, wa, 1536)
    up = part(0, wa, 2048) + part(1, wa, 2560) + part(2, wb, 0) + part(3, wb, 512)
    return (gate / (1.0 + jnp.exp(-gate)) * up).astype(jnp.bfloat16)


def ffn_kernel(x_ref, *refs):
    weights, out_ref, acc_ref, bufs, sems, piece_ref, out_sems = refs[:8], *refs[8:]
    copies = [pltpu.make_async_copy(w, bufs.at[i], sems.at[i]) for i, w in enumerate(weights)]
    for copy in copies:
        copy.start()
    core = lax.axis_index("co")
    leave = []
    for s in range(4):
        copies[2 * s].wait()
        copies[2 * s + 1].wait()
        wa, wb = bufs.at[2 * s], bufs.at[2 * s + 1]
        hidden = slice_hidden(x_ref, wa, wb)
        for c in range(8):
            cols = pl.ds(c * 256, 256)
            term = jnp.dot(
                hidden, wb[pl.ds(1024 + c * 256, 256), :], preferred_element_type=jnp.float32
            )
            total = term if s == 0 else acc_ref[:, cols] + term
            if s < 3:
                acc_ref[:, cols] = total
                continue
            for k in range(2):
                t = 2 * c + k
                place = jnp.where(core == 0, t, (t % 4) * 4 + t // 4)
                piece_ref[t] = total[:, k * 128 : (k + 1) * 128].astype(jnp.bfloat16)
                leave.append(
                    pltpu.make_async_copy(piece_ref.at[t], out_ref.at[place], out_sems.at[t])
                )
                leave[-1].start()
    for copy in leave:
        copy.wait()


def ffn(x, weights):
    return pl.pallas_call(
        ffn_kernel,
        out_shape=pltpu.HBM((16, ROWS_B, 128), jnp.bfloat16),
        in_specs=[VMEM] + [ANY] * 8,
        out_specs=IN_HBM,
        scratch_shapes=[
            pltpu.VMEM((ROWS_B, D), jnp.float32),
            pltpu.VMEM((8, HALF_W, 256), jnp.bfloat16),
            pltpu.SemaphoreType.DMA((8,)),
            pltpu.VMEM((16, ROWS_B, 128), jnp.bfloat16),
            pltpu.SemaphoreType.DMA((16,)),
        ],
        compiler_params=vmem_mib(24),
        name="ffn",
    )(resident(x), *weights)


def total_kernel(parts_ref, out_ref):
    for l in range(4):
        rows = sum(parts_ref[4 * m + l].astype(jnp.float32) for m in range(4))
        out_ref[:, l] = rows.astype(jnp.bfloat16).reshape(EXPERTS, 8, 128)


def total(parts):
    return pl.pallas_call(
        total_kernel,
        out_shape=pltpu.VMEM((EXPERTS, 4, 8, 128), jnp.bfloat16),
        in_specs=[VMEM],
        out_specs=VMEM,
        compiler_params=vmem_mib(8),
        name="total",
    )(resident(parts))


def combine_kernel(ret_ref, slot_ref, weight_ref, out_ref):
    place = lax.broadcasted_iota(jnp.int32, (ROWS_B, EXPERTS * CAP), 1)
    total = None
    for k in range(2):
        pick = jnp.where(place == slot_ref[:, k : k + 1], 1.0, 0.0).astype(jnp.bfloat16)
        rows = jnp.dot(pick, ret_ref[...], preferred_element_type=jnp.float32)
        term = rows * weight_ref[:, k : k + 1]
        total = term if total is None else total + term
    out_ref[...] = total.astype(jnp.bfloat16)


def combine(returned, slots, route_weights):
    return pl.pallas_call(
        combine_kernel,
        out_shape=jax.ShapeDtypeStruct((ROWS_B, 128), jnp.bfloat16),
        in_specs=[VMEM] * 3,
        out_specs=VMEM,
        compiler_params=vmem_mib(12),
        name="combine",
    )(resident(returned), slots, route_weights)


def project_kernel(own_ref, one_ref, two_ref, far_ref, weight_ref, out_ref, a_ref):
    core = lax.axis_index("co")
    line = jnp.where(core == 0, lax.axis_index("x"), lax.axis_index("y"))
    odd = lax.rem(line, 2)
    for ref, source in (
        (own_ref, line),
        (one_ref, line + 1 - 2 * odd),
        (two_ref, 3 - line),
        (far_ref, lax.rem(line + 2, 4)),
    ):
        for m in range(4):
            head = jnp.where(core == 0, m * 4 + source, source * 4 + m)
            a_ref[pl.ds(pl.multiple_of(head * HEAD_DIM, HEAD_DIM), HEAD_DIM), :] = ref[m]
    turned = weight_ref[...].astype(jnp.float32).T.astype(jnp.bfloat16)
    out = jnp.dot(turned, a_ref[...], preferred_element_type=jnp.float32)
    out_ref[...] = out.T.astype(jnp.bfloat16)


def project(own, one, two, far, out_weight):
    return pl.pallas_call(
        project_kernel,
        out_shape=jax.ShapeDtypeStruct((512, 128), jnp.bfloat16),
        in_specs=[VMEM] * 5,
        out_specs=VMEM,
        scratch_shapes=[pltpu.VMEM((1024, 512), jnp.bfloat16)],
        compiler_params=vmem_mib(12),
        name="project",
    )(*(resident(a) for a in (own, one, two, far, out_weight)))


def attend_kernel(q_ref, kv_ref, low_ref, high_ref, cos_ref, sin_ref, sink_ref, out_ref,
                  k_scr, vt_scr):
    half = HEAD_DIM // 2

    def turn(x, rows):
        wide = x.astype(jnp.float32)
        swapped = jnp.concatenate([wide[:, half:], wide[:, :half]], axis=1)
        return (wide * cos_ref[rows, :] + swapped * sin_ref[rows, :]).astype(jnp.bfloat16)

    spans = ((low_ref, 0, HALF_WIN), (kv_ref, HALF_WIN, 512), (high_ref, 512 + HALF_WIN, HALF_WIN))
    for ref, at, count in spans:
        rows = pl.ds(at, count)
        k_scr[rows, :] = turn(ref[0], rows)
        value = ref[1].astype(jnp.float32)
        vt_scr[:, rows] = jnp.concatenate([value, value], axis=1).T.astype(jnp.bfloat16)
    start = (lax.axis_index("z") * 2 + lax.axis_index("co")) * 512
    key_at = lax.broadcasted_iota(jnp.int32, (384, 128), 0) - HALF_WIN
    gap = key_at - lax.broadcasted_iota(jnp.int32, (384, 128), 1)
    sink = sink_ref[0]
    for j in range(4):
        query = turn(q_ref[pl.ds(j * 128, 128), :], pl.ds(HALF_WIN + j * 128, 128))
        scores = lax.dot_general(
            k_scr[pl.ds(j * 128, 384), :], query, (((1,), (1,)), ((), ())),
            preferred_element_type=jnp.float32,
        ) * HEAD_DIM ** (-0.5)
        key = key_at + (start + j * 128)
        allowed = (jnp.abs(gap) <= HALF_WIN) & (key >= 0) & (key < 16384)
        scores = jnp.where(allowed, scores, NEG_BIG)
        peak = jnp.maximum(jnp.max(scores, axis=0, keepdims=True), sink)
        lifted = jnp.exp(scores - peak)
        total = jnp.sum(lifted, axis=0, keepdims=True) + jnp.exp(sink - peak)
        probs = (lifted / total).astype(jnp.bfloat16)
        mixed = jnp.dot(
            vt_scr[pl.ds(0, HEAD_DIM), pl.ds(j * 128, 384)], probs,
            preferred_element_type=jnp.float32,
        )
        out_ref[:, pl.ds(j * 128, 128)] = mixed.astype(jnp.bfloat16)


def attend(query_proj, key_proj, value_proj, sink_logit):
    kv_at = lax.axis_index("y") * HEAD_DIM
    own = jnp.stack(
        [lax.dynamic_slice_in_dim(a, kv_at, HEAD_DIM, 1) for a in (key_proj, value_proj)]
    )
    count = lax.axis_size(EP)
    forward = [(i, i + 1) for i in range(count - 1)]
    backward = [(target, source) for source, target in forward]
    low = lax.ppermute(own[:, 512 - HALF_WIN :], EP, forward)
    high = lax.ppermute(own[:, :HALF_WIN], EP, backward)
    offset = lax.axis_index(EP) * 512 - HALF_WIN
    half = HEAD_DIM // 2
    channel = jnp.arange(HEAD_DIM, dtype=jnp.int32)
    inverse_freq = 1.0 / ROPE_BASE ** ((channel % half).astype(jnp.float32) * 2.0 / HEAD_DIM)
    position = (jnp.arange(512 + 2 * HALF_WIN, dtype=jnp.int32) + offset).astype(jnp.float32)
    angles = position[:, None] * inverse_freq[None, :]
    cosine = jnp.cos(angles)
    sine = jnp.where(channel < half, -1.0, 1.0)[None, :] * jnp.sin(angles)
    return pl.pallas_call(
        attend_kernel,
        out_shape=jax.ShapeDtypeStruct((HEAD_DIM, 512), jnp.bfloat16),
        in_specs=[VMEM] * 6 + [pl.BlockSpec(memory_space=pltpu.SMEM)],
        out_specs=VMEM,
        scratch_shapes=[
            pltpu.VMEM((768, HEAD_DIM), jnp.bfloat16), pltpu.VMEM((128, 768), jnp.bfloat16)
        ],
        compiler_params=vmem_mib(12),
        name="attend",
    )(*(resident(a) for a in (query_proj, own, low, high, cosine, sine)), sink_logit)


def local(
    query_proj,
    key_proj,
    value_proj,
    sink_logit,
    out_weight,
    expert_input,
    norm_gain,
    routes,
    route_weights,
    gate_weight,
    up_weight,
    down_weight,
):
    wa, wb = pack(gate_weight, up_weight, down_weight)
    one_a = swap(wa, NEAR_A)
    two_b = swap(wb, NEAR_B)
    one_b = swap(wb, NEAR_A)
    two_a = swap(wa, NEAR_B)
    outgoing, slots = prepare(expert_input, norm_gain, routes)
    arrived = lax.all_to_all(outgoing, EP, 0, 0, tiled=True)
    far_a = swap(one_a, NEAR_B)
    far_b = swap(two_b, NEAR_A)

    attended = attend(query_proj, key_proj, value_proj, sink_logit)

    payload = jnp.concatenate([arrived, attended], axis=0)
    rows = lax.all_to_all(
        jnp.broadcast_to(payload[None], (4, *payload.shape)),
        PLANE, 0, 0, tiled=True, axis_index_groups=LINE_M,
    )
    partial = ffn(rows, (wa, wb, one_a, one_b, two_a, two_b, far_a, far_b))
    parts = lax.all_to_all(partial, PLANE, 0, 0, tiled=True, axis_index_groups=WHOLE)
    result = total(parts).reshape(EXPERTS, CAP, 128)
    returned = lax.all_to_all(result, EP, 0, 0, tiled=True)
    expert_out = combine(returned.reshape(EXPERTS * CAP, 128), slots, route_weights)

    heads = rows[:, 256:]
    one = swap(heads, NEAR_A)
    far = swap(heads, ACROSS)
    two = swap(heads, NEAR_B)
    mixer_out = project(heads, one, two, far, out_weight)
    return (mixer_out, expert_out)


def solution(mesh):
    finer = Mesh(mesh.devices.reshape(16, 2, 4, 4), ("z", "co", "y", "x"))
    in_specs = (
        P(EP, TP),
        P(EP, None),
        P(EP, None),
        P(TP),
        P(None, TP),
        P(EP, None),
        P(),
        P(EP, None),
        P(EP, None),
        P(EP, None, TP),
        P(EP, None, TP),
        P(EP, TP, None),
    )
    out_specs = (P(EP, TP), P(EP, TP))
    return jax.shard_map(local, mesh=finer, in_specs=in_specs, out_specs=out_specs, check_vma=False)
```

```python
import jax
import jax.numpy as jnp
from jax import lax
from jax.experimental import pallas as pl
from jax.experimental.pallas import tpu as pltpu
from jax.sharding import Mesh
from jax.sharding import PartitionSpec as P


D = 2048
HEAD_DIM = 64
HALF_WIN = 128
ROWS_B = 256
EXPERTS = 32
CAP = 32
EP = ("z", "co")
TP = ("y", "x")
PLANE = ("co", "y", "x")

NORM_EPS = 1e-06
ROPE_BASE = 10000.0
NEG_BIG = -1e30

LINE_L = [[y * 4 + x for x in range(4)] for y in range(4)] + [
    [16 + y * 4 + x for y in range(4)] for x in range(4)
]
LINE_M = [[y * 4 + x for y in range(4)] for x in range(4)] + [
    [16 + y * 4 + x for x in range(4)] for y in range(4)
]
WHOLE = [list(range(16)), [16 + (p % 4) * 4 + p // 4 for p in range(16)]]


ANY = pl.BlockSpec(memory_space=pl.ANY)
VMEM = pl.BlockSpec(memory_space=pltpu.VMEM)
IN_HBM = pl.BlockSpec(memory_space=pltpu.HBM)
HALF_W = 3072


def resident(x):
    return pltpu.with_memory_space_constraint(x, pltpu.VMEM)


def in_hbm(x):
    return pltpu.with_memory_space_constraint(x, pltpu.HBM)


def vmem_mib(count):
    return pltpu.CompilerParams(vmem_limit_bytes=count << 20)


NEAR_A = (1, 0, 3, 2)
NEAR_B = (3, 2, 1, 0)
ACROSS = (2, 3, 0, 1)


def swap(x, partner):
    pairs = [(line[i], line[partner[i]]) for line in LINE_L for i in range(4)]
    return lax.ppermute(x, PLANE, pairs)


def pack_kernel(gate_ref, up_ref, down_ref, wa_ref, wb_ref, stage_ref, sems, out_sems):
    second = [(up_ref.at[0, pl.ds(1024, 1024)], 0, 1024)] + [
        (down_ref.at[0, :, pl.ds(c * 256, 256)], 1024 + c * 256, 256) for c in range(8)
    ]
    come = [
        pltpu.make_async_copy(source, stage_ref.at[pl.ds(at, count)], sems.at[i])
        for i, (source, at, count) in enumerate(second)
    ]
    leave = [
        pltpu.make_async_copy(
            stage_ref.at[pl.ds(at, count)], wb_ref.at[pl.ds(at, count)], out_sems.at[i]
        )
        for i, (_, at, count) in enumerate(second)
    ]
    first = [
        pltpu.make_async_copy(gate_ref.at[0], wa_ref.at[pl.ds(0, 2048)], sems.at[9]),
        pltpu.make_async_copy(
            up_ref.at[0, pl.ds(0, 1024)], wa_ref.at[pl.ds(2048, 1024)], sems.at[10]
        ),
    ]
    for copy in come + first:
        copy.start()
    for arrival, departure in zip(come, leave):
        arrival.wait()
        departure.start()
    for copy in first + leave:
        copy.wait()


def pack(gate, up, down):
    return pl.pallas_call(
        pack_kernel,
        out_shape=(
            pltpu.VMEM((HALF_W, 256), jnp.bfloat16), pltpu.HBM((HALF_W, 256), jnp.bfloat16)
        ),
        in_specs=[IN_HBM] * 3,
        out_specs=(VMEM, IN_HBM),
        scratch_shapes=[
            pltpu.VMEM((HALF_W, 256), jnp.bfloat16),
            pltpu.SemaphoreType.DMA((11,)),
            pltpu.SemaphoreType.DMA((9,)),
        ],
        compiler_params=vmem_mib(8),
        name="pack",
    )(*(in_hbm(a) for a in (gate, up, down)))


def prep_kernel(x_ref, gain_ref, routes_ref, out_ref, slot_ref, normed_ref):
    def norm_rows(i, carry):
        rows = pl.ds(pl.multiple_of(i * 32, 32), 32)
        wide = x_ref[rows, :].astype(jnp.float32)
        scale = lax.rsqrt(jnp.mean(wide * wide, axis=1, keepdims=True) + NORM_EPS)
        normed_ref[rows, :] = (wide * scale * gain_ref[...]).astype(jnp.bfloat16)
        return carry

    lax.fori_loop(0, ROWS_B // 32, norm_rows, 0)

    first = routes_ref[0:1, :]
    second = routes_ref[1:2, :]
    expert = lax.broadcasted_iota(jnp.int32, (128, ROWS_B), 0)
    row = lax.broadcasted_iota(jnp.int32, (ROWS_B, ROWS_B), 0)
    col = lax.broadcasted_iota(jnp.int32, (ROWS_B, ROWS_B), 1)
    above = jnp.where(row < col, 1.0, 0.0).astype(jnp.bfloat16)
    named = jnp.where((first == expert) | (second == expert), 1.0, 0.0)
    rank = jnp.dot(named.astype(jnp.bfloat16), above, preferred_element_type=jnp.float32)
    rank_a = jnp.sum(jnp.where(first == expert, rank, 0.0), axis=0, keepdims=True)
    rank_b = jnp.sum(jnp.where(second == expert, rank, 0.0), axis=0, keepdims=True)
    slot_a = first * CAP + rank_a.astype(jnp.int32)
    slot_b = second * CAP + rank_b.astype(jnp.int32)
    both = jnp.where(expert == 0, slot_a, slot_b).astype(jnp.float32)
    slot_ref[...] = both.T.astype(jnp.int32)

    mark = jnp.where(named > 0.5, rank, -1.0).astype(jnp.bfloat16)
    spread = jnp.where(
        (lax.broadcasted_iota(jnp.int32, (ROWS_B, 128), 0) >> 3)
        == lax.broadcasted_iota(jnp.int32, (ROWS_B, 128), 1),
        1.0,
        0.0,
    ).astype(jnp.bfloat16)
    mark_rows = jnp.dot(spread, mark, preferred_element_type=jnp.float32)
    xi = lax.axis_index("x")
    yi = lax.axis_index("y")
    even = ((row >> 3) & 1) == 0
    wanted = jnp.where(even, xi, yi) * 8 + (row & 7)
    pick = jnp.where(mark_rows.astype(jnp.int32) == wanted, 1.0, 0.0).astype(jnp.bfloat16)
    from_y = jnp.dot(
        pick, normed_ref[:, pl.ds(pl.multiple_of(yi * 512, 512), 512)],
        preferred_element_type=jnp.float32,
    )
    from_x = jnp.dot(
        pick, normed_ref[:, pl.ds(pl.multiple_of(xi * 512, 512), 512)],
        preferred_element_type=jnp.float32,
    )
    even_row = ((lax.broadcasted_iota(jnp.int32, (ROWS_B, 512), 0) >> 3) & 1) == 0
    out_ref[...] = jnp.where(even_row, from_y, from_x).astype(jnp.bfloat16)


def prepare(expert_input, norm_gain, routes):
    return pl.pallas_call(
        prep_kernel,
        out_shape=(
            jax.ShapeDtypeStruct((ROWS_B, 512), jnp.bfloat16),
            jax.ShapeDtypeStruct((ROWS_B, 128), jnp.int32),
        ),
        in_specs=[VMEM] * 3,
        out_specs=(VMEM, VMEM),
        scratch_shapes=[pltpu.VMEM((ROWS_B, D), jnp.bfloat16)],
        compiler_params=vmem_mib(16),
        name="prep",
    )(expert_input, norm_gain.reshape(1, D), routes.T)


def slice_hidden(x_ref, wa, wb):
    def part(m, ref, start):
        return jnp.dot(
            x_ref[m, pl.ds(0, ROWS_B), :], ref[pl.ds(start, 512), :],
            preferred_element_type=jnp.float32,
        )

    gate = part(0, wa, 0) + part(1, wa, 512) + part(2, wa, 1024) + part(3, wa, 1536)
    up = part(0, wa, 2048) + part(1, wa, 2560) + part(2, wb, 0) + part(3, wb, 512)
    return (gate / (1.0 + jnp.exp(-gate)) * up).astype(jnp.bfloat16)


def ffn_kernel(x_ref, *refs):
    weights, out_ref, acc_ref, bufs, sems, piece_ref, out_sems = refs[:8], *refs[8:]
    copies = [pltpu.make_async_copy(w, bufs.at[i], sems.at[i]) for i, w in enumerate(weights)]
    for copy in copies:
        copy.start()
    core = lax.axis_index("co")
    leave = []
    for s in range(4):
        copies[2 * s].wait()
        copies[2 * s + 1].wait()
        wa, wb = bufs.at[2 * s], bufs.at[2 * s + 1]
        hidden = slice_hidden(x_ref, wa, wb)
        for c in range(8):
            cols = pl.ds(c * 256, 256)
            term = jnp.dot(
                hidden, wb[pl.ds(1024 + c * 256, 256), :], preferred_element_type=jnp.float32
            )
            total = term if s == 0 else acc_ref[:, cols] + term
            if s < 3:
                acc_ref[:, cols] = total
                continue
            for k in range(2):
                t = 2 * c + k
                place = jnp.where(core == 0, t, (t % 4) * 4 + t // 4)
                piece_ref[t] = total[:, k * 128 : (k + 1) * 128].astype(jnp.bfloat16)
                leave.append(
                    pltpu.make_async_copy(piece_ref.at[t], out_ref.at[place], out_sems.at[t])
                )
                leave[-1].start()
    for copy in leave:
        copy.wait()


def ffn(x, weights):
    return pl.pallas_call(
        ffn_kernel,
        out_shape=pltpu.HBM((16, ROWS_B, 128), jnp.bfloat16),
        in_specs=[VMEM, ANY] + [IN_HBM] * 7,
        out_specs=IN_HBM,
        scratch_shapes=[
            pltpu.VMEM((ROWS_B, D), jnp.float32),
            pltpu.VMEM((8, HALF_W, 256), jnp.bfloat16),
            pltpu.SemaphoreType.DMA((8,)),
            pltpu.VMEM((16, ROWS_B, 128), jnp.bfloat16),
            pltpu.SemaphoreType.DMA((16,)),
        ],
        compiler_params=vmem_mib(24),
        name="ffn",
    )(resident(x), weights[0], *(in_hbm(a) for a in weights[1:]))


def total_kernel(parts_ref, out_ref):
    for l in range(4):
        rows = sum(parts_ref[4 * m + l].astype(jnp.float32) for m in range(4))
        out_ref[:, l] = rows.astype(jnp.bfloat16).reshape(EXPERTS, 8, 128)


def total(parts):
    return pl.pallas_call(
        total_kernel,
        out_shape=pltpu.VMEM((EXPERTS, 4, 8, 128), jnp.bfloat16),
        in_specs=[VMEM],
        out_specs=VMEM,
        compiler_params=vmem_mib(8),
        name="total",
    )(resident(parts))


def combine_kernel(ret_ref, slot_ref, weight_ref, out_ref):
    place = lax.broadcasted_iota(jnp.int32, (ROWS_B, EXPERTS * CAP), 1)
    total = None
    for k in range(2):
        pick = jnp.where(place == slot_ref[:, k : k + 1], 1.0, 0.0).astype(jnp.bfloat16)
        rows = jnp.dot(pick, ret_ref[...], preferred_element_type=jnp.float32)
        term = rows * weight_ref[:, k : k + 1]
        total = term if total is None else total + term
    out_ref[...] = total.astype(jnp.bfloat16)


def combine(returned, slots, route_weights):
    return pl.pallas_call(
        combine_kernel,
        out_shape=jax.ShapeDtypeStruct((ROWS_B, 128), jnp.bfloat16),
        in_specs=[VMEM] * 3,
        out_specs=VMEM,
        compiler_params=vmem_mib(12),
        name="combine",
    )(resident(returned), slots, route_weights)


def project_kernel(own_ref, one_ref, two_ref, far_ref, weight_ref, out_ref, a_ref):
    core = lax.axis_index("co")
    line = jnp.where(core == 0, lax.axis_index("x"), lax.axis_index("y"))
    odd = lax.rem(line, 2)
    for ref, source in (
        (own_ref, line),
        (one_ref, line + 1 - 2 * odd),
        (two_ref, 3 - line),
        (far_ref, lax.rem(line + 2, 4)),
    ):
        for m in range(4):
            head = jnp.where(core == 0, m * 4 + source, source * 4 + m)
            a_ref[pl.ds(pl.multiple_of(head * HEAD_DIM, HEAD_DIM), HEAD_DIM), :] = ref[m]
    turned = weight_ref[...].astype(jnp.float32).T.astype(jnp.bfloat16)
    out = jnp.dot(turned, a_ref[...], preferred_element_type=jnp.float32)
    out_ref[...] = out.T.astype(jnp.bfloat16)


def project(own, one, two, far, out_weight):
    return pl.pallas_call(
        project_kernel,
        out_shape=jax.ShapeDtypeStruct((512, 128), jnp.bfloat16),
        in_specs=[VMEM] * 5,
        out_specs=VMEM,
        scratch_shapes=[pltpu.VMEM((1024, 512), jnp.bfloat16)],
        compiler_params=vmem_mib(12),
        name="project",
    )(*(resident(a) for a in (own, one, two, far, out_weight)))


def attend_kernel(q_ref, kv_ref, low_ref, high_ref, cos_ref, sin_ref, sink_ref, out_ref,
                  k_scr, vt_scr):
    half = HEAD_DIM // 2

    def turn(x, rows):
        wide = x.astype(jnp.float32)
        swapped = jnp.concatenate([wide[:, half:], wide[:, :half]], axis=1)
        return (wide * cos_ref[rows, :] + swapped * sin_ref[rows, :]).astype(jnp.bfloat16)

    spans = ((low_ref, 0, HALF_WIN), (kv_ref, HALF_WIN, 512), (high_ref, 512 + HALF_WIN, HALF_WIN))
    for ref, at, count in spans:
        rows = pl.ds(at, count)
        k_scr[rows, :] = turn(ref[0], rows)
        value = ref[1].astype(jnp.float32)
        vt_scr[:, rows] = jnp.concatenate([value, value], axis=1).T.astype(jnp.bfloat16)
    start = (lax.axis_index("z") * 2 + lax.axis_index("co")) * 512
    key_at = lax.broadcasted_iota(jnp.int32, (384, 128), 0) - HALF_WIN
    gap = key_at - lax.broadcasted_iota(jnp.int32, (384, 128), 1)
    sink = sink_ref[0]
    for j in range(4):
        query = turn(q_ref[pl.ds(j * 128, 128), :], pl.ds(HALF_WIN + j * 128, 128))
        scores = lax.dot_general(
            k_scr[pl.ds(j * 128, 384), :], query, (((1,), (1,)), ((), ())),
            preferred_element_type=jnp.float32,
        ) * HEAD_DIM ** (-0.5)
        key = key_at + (start + j * 128)
        allowed = (jnp.abs(gap) <= HALF_WIN) & (key >= 0) & (key < 16384)
        scores = jnp.where(allowed, scores, NEG_BIG)
        peak = jnp.maximum(jnp.max(scores, axis=0, keepdims=True), sink)
        lifted = jnp.exp(scores - peak)
        total = jnp.sum(lifted, axis=0, keepdims=True) + jnp.exp(sink - peak)
        probs = (lifted / total).astype(jnp.bfloat16)
        mixed = jnp.dot(
            vt_scr[pl.ds(0, HEAD_DIM), pl.ds(j * 128, 384)], probs,
            preferred_element_type=jnp.float32,
        )
        out_ref[:, pl.ds(j * 128, 128)] = mixed.astype(jnp.bfloat16)


def attend(query_proj, key_proj, value_proj, sink_logit):
    kv_at = lax.axis_index("y") * HEAD_DIM
    own = jnp.stack(
        [lax.dynamic_slice_in_dim(a, kv_at, HEAD_DIM, 1) for a in (key_proj, value_proj)]
    )
    count = lax.axis_size(EP)
    forward = [(i, i + 1) for i in range(count - 1)]
    backward = [(target, source) for source, target in forward]
    low = lax.ppermute(own[:, 512 - HALF_WIN :], EP, forward)
    high = lax.ppermute(own[:, :HALF_WIN], EP, backward)
    offset = lax.axis_index(EP) * 512 - HALF_WIN
    half = HEAD_DIM // 2
    channel = jnp.arange(HEAD_DIM, dtype=jnp.int32)
    inverse_freq = 1.0 / ROPE_BASE ** ((channel % half).astype(jnp.float32) * 2.0 / HEAD_DIM)
    position = (jnp.arange(512 + 2 * HALF_WIN, dtype=jnp.int32) + offset).astype(jnp.float32)
    angles = position[:, None] * inverse_freq[None, :]
    cosine = jnp.cos(angles)
    sine = jnp.where(channel < half, -1.0, 1.0)[None, :] * jnp.sin(angles)
    return pl.pallas_call(
        attend_kernel,
        out_shape=jax.ShapeDtypeStruct((HEAD_DIM, 512), jnp.bfloat16),
        in_specs=[VMEM] * 6 + [pl.BlockSpec(memory_space=pltpu.SMEM)],
        out_specs=VMEM,
        scratch_shapes=[
            pltpu.VMEM((768, HEAD_DIM), jnp.bfloat16), pltpu.VMEM((128, 768), jnp.bfloat16)
        ],
        compiler_params=vmem_mib(12),
        name="attend",
    )(*(resident(a) for a in (query_proj, own, low, high, cosine, sine)), sink_logit)


def local(
    query_proj,
    key_proj,
    value_proj,
    sink_logit,
    out_weight,
    expert_input,
    norm_gain,
    routes,
    route_weights,
    gate_weight,
    up_weight,
    down_weight,
):
    wa, wb = pack(gate_weight, up_weight, down_weight)
    one_a = swap(wa, NEAR_A)
    two_b = swap(wb, NEAR_B)
    two_a = swap(wa, NEAR_B)
    one_b = swap(wb, NEAR_A)
    outgoing, slots = prepare(expert_input, norm_gain, routes)
    arrived = lax.all_to_all(outgoing, EP, 0, 0, tiled=True)
    far_a = swap(one_a, NEAR_B)
    far_b = swap(two_b, NEAR_A)

    attended = attend(query_proj, key_proj, value_proj, sink_logit)

    payload = jnp.concatenate([arrived, attended], axis=0)
    rows = lax.all_to_all(
        jnp.broadcast_to(payload[None], (4, *payload.shape)),
        PLANE, 0, 0, tiled=True, axis_index_groups=LINE_M,
    )
    partial = ffn(rows, (wa, wb, one_a, one_b, two_a, two_b, far_a, far_b))
    parts = lax.all_to_all(partial, PLANE, 0, 0, tiled=True, axis_index_groups=WHOLE)
    result = total(parts).reshape(EXPERTS, CAP, 128)
    returned = lax.all_to_all(result, EP, 0, 0, tiled=True)
    expert_out = combine(returned.reshape(EXPERTS * CAP, 128), slots, route_weights)

    heads = rows[:, 256:]
    near = [swap(heads, partner) for partner in (NEAR_A, NEAR_B)]
    far = swap(heads, ACROSS)
    mixer_out = project(heads, *near, far, out_weight)
    return (mixer_out, expert_out)


def solution(mesh):
    finer = Mesh(mesh.devices.reshape(16, 2, 4, 4), ("z", "co", "y", "x"))
    in_specs = (
        P(EP, TP),
        P(EP, None),
        P(EP, None),
        P(TP),
        P(None, TP),
        P(EP, None),
        P(),
        P(EP, None),
        P(EP, None),
        P(EP, None, TP),
        P(EP, None, TP),
        P(EP, TP, None),
    )
    out_specs = (P(EP, TP), P(EP, TP))
    return jax.shard_map(local, mesh=finer, in_specs=in_specs, out_specs=out_specs, check_vma=False)
```
